256 devices in a mesh: dp: 4 (over x), kv: 32 (over z, y), tp: 2 (over core).
Axes of the slice: x: 4, y: 4, z: 8, core: 2. Of those that a mesh axis runs over, the one named last changes fastest.
Arguments:
- tokens: bfloat16 [64, 16, 4096], P('dp', None, 'kv'), may hold values from -64 to 64
- in_gain: bfloat16 [4096], P('kv'), may hold values from 0.099609375 to 1.8984375
- query_weight: bfloat16 [4096, 4096], P('kv', 'tp'), may hold values from -0.125 to 0.125
- key_weight: bfloat16 [4096, 4096], P('kv', 'tp'), may hold values from -0.125 to 0.125
- value_weight: bfloat16 [4096, 4096], P('kv', 'tp'), may hold values from -0.09375 to 0.09375
- out_weight: bfloat16 [4096, 4096], P('tp', 'kv'), may hold values from -0.1875 to 0.1875
- lambdas: float32 [16], P('tp'), may hold values from 0.3 to 0.8
- sub_gain: bfloat16 [256], replicated, may hold values from 0.099609375 to 1.8984375
- key_cache: bfloat16 [64, 1024, 16, 2, 128], P('dp', 'kv', 'tp'), may hold values from -248 to 248
- value_cache: bfloat16 [64, 1024, 16, 256], P('dp', 'kv', 'tp'), may hold values from -6 to 6
- cache_len: int32 [64], P('dp'), may hold values from 512 to 992
- accepted: int32 [64], P('dp'), may hold values from 0 to 16
- parents: int32 [64, 16], P('dp'), may hold values from -1 to 14, as said below
Outputs:
- output: bfloat16 [64, 16, 4096], P('dp', None, ('kv', 'tp'))
- key_cache_out: bfloat16 [64, 1024, 16, 2, 128], P('dp', 'kv', 'tp')
- value_cache_out: bfloat16 [64, 1024, 16, 256], P('dp', 'kv', 'tp')
The draws below stay inside these ranges and needn't reach their ends.
Inputs may be any that keep to these rules, and one draw needn't show every extreme that they name: `parents`: each proposal's parent is -1 (the text already in the cache) or one of the three proposals just before it; the last proposal's parent is the one just before it. Positions below cache_len plus accepted hold a sequence's text; the later ones are stale.
All inputs are finite; a program needn't handle non-finite values.
Results may differ from the reference program's by a relative error of at most 0.019.
The reference program's roundings to bfloat16 on the way count: a program that leaves them out, or rounds other values in their place, can miss the bound.
Values may be sent and summed in bfloat16 or wider, within the bound.
A program may use at most 64 MiB of HBM per device.

```python
import math
import jax
import jax.numpy as jnp
from jax import lax

D = 4096
HD = 128
H = 16
P_SIZE = 16
POS_DEV = 32
BATCH = 64
LEN = 1024
N_TP = 2


def draw_tokens(key, part):
    key_one = jax.random.fold_in(key, 0)
    column = 10.0 ** (jnp.arange(D, dtype=jnp.float32) / D)
    values = jax.random.normal(key_one, (BATCH, P_SIZE, D), jnp.float32) * column
    return jnp.clip(values, -64.0, 64.0).astype(jnp.bfloat16)


def draw_key_cache(key, part):
    key_one = jax.random.fold_in(key, 0)
    noise = jnp.clip(jax.random.normal(key_one, (BATCH, LEN, H, 2, HD), jnp.float32) * 1.3, -8.0, 8.0)
    return noise.astype(jnp.bfloat16)


def draw_parents(key, part):
    step_back = jax.random.randint(key, (BATCH, P_SIZE), 0, 3)
    last_column = (jnp.arange(P_SIZE, dtype=jnp.int32) == P_SIZE - 1)[None, :]
    step_back = jnp.where(last_column, 0, step_back)
    return jnp.maximum(jnp.arange(P_SIZE, dtype=jnp.int32)[None, :] - 1 - step_back, -1).astype(jnp.int32)


def place_ends(result, own_key, least, largest):
    longest = result.shape.index(max(result.shape))
    spots = []
    for shift in (0, 1):
        where = [jax.random.randint(jax.random.fold_in(own_key, axis), (), 0, length) for axis, length in enumerate(result.shape)]
        where[longest] = (where[longest] + shift) % result.shape[longest]
        spots.append(tuple(where))
    return result.at[spots[0]].set(least).at[spots[1]].set(largest)


def levels(stream_key, extent, shards, smallest, high):
    def one(position, blocks):
        draws = jax.random.uniform(jax.random.fold_in(jax.random.fold_in(stream_key, 6), position), (blocks,), jnp.float32, smallest / len(shards), high / len(shards))
        return jnp.repeat(jnp.exp(draws), extent[position] // blocks).reshape((-1,) + (1,) * (len(extent) - position - 1))

    loudness = one(*shards[0])
    for cut in shards[1:]:
        loudness = loudness * one(*cut)
    return loudness


def gaussian(key, dims, deviation, most, pieces=(), kind=jnp.bfloat16):
    values = deviation * jax.random.normal(key, dims, jnp.float32)
    if pieces:
        values = values * levels(key, dims, pieces, -0.22, 0.18)
    return jnp.clip(values, -most, most).astype(kind)


def setup_inputs(seed: int = 0) -> dict:
    key_list = jax.random.split(jax.random.key(seed), 14)
    return {
        "tokens": draw_tokens(jax.random.fold_in(key_list[13], 71), 0),
        "in_gain": jnp.clip(1.0 + 0.18 * jax.random.normal(key_list[1], (D,), jnp.float32), 0.099609375, 1.8984375).astype(jnp.bfloat16),
        "query_weight": gaussian(key_list[2], (D, D), (D * 10 // 17) ** -0.5, 0.125, ((0, 32), (1, 2))),
        "key_weight": gaussian(key_list[3], (D, D), (D * 10 // 17) ** -0.5, 0.125, ((0, 32), (1, 2))),
        "value_weight": gaussian(key_list[4], (D, D), D ** -0.5, 0.09375, ((0, 32), (1, 2))),
        "out_weight": gaussian(key_list[5], (D, D), (D // 4) ** -0.5, 0.1875, ((0, 2), (1, 32))),
        "lambdas": jnp.clip(0.3 + 0.5 * jax.random.uniform(key_list[6], (H,), jnp.float32) ** levels(key_list[6], (H,), ((0, 2),), -0.2, 0.2), 0.3, 0.8),
        "sub_gain": jnp.clip(1.0 + 0.18 * jax.random.normal(key_list[7], (2 * HD,), jnp.float32), 0.099609375, 1.8984375).astype(jnp.bfloat16),
        "key_cache": draw_key_cache(jax.random.fold_in(key_list[13], 71), 0),
        "value_cache": gaussian(key_list[9], (BATCH, LEN, H, 2 * HD), 1.0, 6.0, ((0, 4), (1, 32), (2, 2))),
        "cache_len": place_ends(jax.random.randint(key_list[10], (BATCH,), LEN // 2, LEN - 2 * P_SIZE + 1), jax.random.fold_in(key_list[10], 1), LEN // 2, LEN - 2 * P_SIZE).astype(jnp.int32),
        "accepted": place_ends(jax.random.randint(key_list[11], (BATCH,), 0, P_SIZE + 1), jax.random.fold_in(key_list[11], 1), 0, P_SIZE).astype(jnp.int32),
        "parents": draw_parents(jax.random.fold_in(key_list[13], 71), 0),
    }


LAMBDA_SCALE = 0.2 + 0.6 * math.exp(-0.6)
NEG_FILL = -1e+30

def visible_links(parents):
    number = parents.shape[-1]
    identity = jnp.eye(number, dtype=jnp.float32)
    parent_links = (parents[..., :, None] == jnp.arange(number, dtype=jnp.int32)[None, :]).astype(jnp.float32)

    def extend(repeat, reached):
        return jnp.maximum(identity, jnp.einsum('bij,bjk->bik', parent_links, reached, precision=lax.Precision.HIGHEST))
    reached = lax.fori_loop(0, number, extend, jnp.broadcast_to(identity, parent_links.shape))
    depths = (lax.optimization_barrier(jnp.sum(reached, axis=-1)) - 1.0).astype(jnp.int32)
    return (reached > 0.5, depths)

def rotate(values, positions):
    half_dim = values.shape[-1] // 2
    frequency = 10000.0 ** (-jnp.arange(half_dim, dtype=jnp.float32) / half_dim)
    angles = positions.astype(jnp.float32)[..., None] * frequency
    cosine = jnp.cos(angles)[..., None, None, :]
    sine_part = jnp.sin(angles)[..., None, None, :]
    lower_half = values[..., :half_dim]
    upper_half = values[..., half_dim:]
    return jnp.concatenate([lower_half * cosine - upper_half * sine_part, upper_half * cosine + lower_half * sine_part], axis=-1)

def reference(tokens, in_gain, query_weight, key_weight, value_weight, out_weight, lambdas, sub_gain, key_cache, value_cache, cache_len, accepted, parents):
    batch_size, prop_count, width_all = tokens.shape
    head_count = lambdas.shape[0]
    head_dim = key_cache.shape[-1]
    tokens_wide = tokens.astype(jnp.float32)
    squares = lax.optimization_barrier(jnp.sum(tokens_wide * tokens_wide, axis=-1))
    row_scale = lax.rsqrt(squares / width_all + 1e-06)[..., None]
    normed = (tokens_wide * in_gain.astype(jnp.float32)).astype(jnp.bfloat16).reshape(batch_size * prop_count, width_all)
    starts = cache_len + accepted
    visible, depths = visible_links(parents)
    positions = starts[:, None] + depths

    def project(weight):
        product = jnp.dot(normed, weight, preferred_element_type=jnp.float32)
        return product.reshape(batch_size, prop_count, -1) * row_scale
    vec_shape = (batch_size, prop_count, head_count, 2, head_dim)
    queries = rotate(project(query_weight).reshape(vec_shape), positions).astype(jnp.bfloat16)
    new_keys = rotate(project(key_weight).reshape(vec_shape), positions).astype(jnp.bfloat16)
    new_values = project(value_weight).reshape(batch_size, prop_count, head_count, 2 * head_dim).astype(jnp.bfloat16)
    slot_index = starts[:, None] + jnp.arange(prop_count, dtype=jnp.int32)[None, :]
    seq_index = jnp.broadcast_to(jnp.arange(batch_size, dtype=jnp.int32)[:, None], slot_index.shape)
    key_out = key_cache.at[seq_index, slot_index].set(new_keys)
    value_out = value_cache.at[seq_index, slot_index].set(new_values)
    lam_mix = lambdas[:, None, None]
    inverse_root = head_dim ** (-0.5)

    def one_sequence(sequence_items):
        query_rows, key_new, value_new, key_rows, value_rows, start_pos, seen_mask = sequence_items
        length = key_rows.shape[0]
        query_wide = query_rows.astype(jnp.float32)
        cache_scores = jnp.einsum('qhmd,thmd->hmqt', query_wide, key_rows.astype(jnp.float32)) * inverse_root
        live_mask = (jnp.arange(length, dtype=jnp.int32) < start_pos)[None, None, None, :]
        cache_scores = jnp.where(live_mask, cache_scores, NEG_FILL)
        own_scores = jnp.einsum('qhmd,jhmd->hmqj', query_wide, key_new.astype(jnp.float32)) * inverse_root
        own_mask = seen_mask[None, None]
        own_scores = jnp.where(own_mask, own_scores, NEG_FILL)
        highest = jnp.maximum(lax.optimization_barrier(jnp.max(cache_scores, axis=-1)), lax.optimization_barrier(jnp.max(own_scores, axis=-1)))
        cache_exp = jnp.where(live_mask, jnp.exp(cache_scores - highest[..., None]), 0.0)
        own_exp = jnp.where(own_mask, jnp.exp(own_scores - highest[..., None]), 0.0)
        totals = lax.optimization_barrier(jnp.sum(cache_exp, axis=-1)) + lax.optimization_barrier(jnp.sum(own_exp, axis=-1))
        cache_prob = cache_exp / totals[..., None]
        own_prob = own_exp / totals[..., None]
        cache_weight = (cache_prob[:, 0] - lam_mix * cache_prob[:, 1]).astype(jnp.bfloat16)
        own_weight = (own_prob[:, 0] - lam_mix * own_prob[:, 1]).astype(jnp.bfloat16)
        blocks = length // POS_DEV
        block_weight = cache_weight.reshape(head_count, prop_count, blocks, POS_DEV).astype(jnp.float32)
        block_values = value_rows.reshape(blocks, POS_DEV, head_count, 2 * head_dim).astype(jnp.float32)
        partial_value = jnp.einsum('hqnt,nthe->nqhe', block_weight, block_values)
        partial_value = lax.optimization_barrier(partial_value.astype(jnp.bfloat16)).astype(jnp.float32)
        own_term = jnp.einsum('hqj,jhe->qhe', own_weight.astype(jnp.float32), value_new.astype(jnp.float32))
        return lax.optimization_barrier(jnp.sum(partial_value, axis=0)) + own_term
    attended = lax.map(one_sequence, (queries, new_keys, new_values, key_cache, value_cache, starts, visible))
    mixed_out = attended * lax.rsqrt(lax.optimization_barrier(jnp.mean(attended * attended, axis=-1, keepdims=True)) + 1e-05)
    mixed_out = (mixed_out * sub_gain.astype(jnp.float32) * LAMBDA_SCALE).astype(jnp.bfloat16)
    mixed_out = mixed_out.reshape(batch_size * prop_count, head_count * 2 * head_dim)
    group_cols = head_count * 2 * head_dim // N_TP
    totals_out = jnp.zeros((batch_size * prop_count, width_all), jnp.float32)
    for member in range(N_TP):
        product = jnp.dot(mixed_out[:, member * group_cols:(member + 1) * group_cols], out_weight[member * group_cols:(member + 1) * group_cols], preferred_element_type=jnp.float32)
        totals_out = totals_out + lax.optimization_barrier(product.astype(jnp.bfloat16)).astype(jnp.float32)
    output = totals_out.astype(jnp.bfloat16).reshape(batch_size, prop_count, width_all)
    return (output, key_out, value_out)
```

```python
import functools
import math

import jax
import jax.numpy as jnp
from jax import lax
from jax.experimental import pallas as pl
from jax.experimental.pallas import tpu as pltpu
from jax.sharding import Mesh
from jax.sharding import PartitionSpec as P

D = 4096
NZ, NY = 8, 4
KV = ("kv_0", "kv_1")
KV_TP = ("kv_0", "kv_1", "tp")
LAMBDA_SCALE = 0.2 + 0.6 * math.exp(-0.6)
NEG_FILL = -1e30
ROOT = 128 ** (-0.5)
F32, BF16 = jnp.float32, jnp.bfloat16
MESH_ID = pl.DeviceIdType.MESH
DMA = pltpu.SemaphoreType.DMA
Z_STEPS = (1, 7, 2, 6, 3, 5, 4)
Y_STEPS = (1, 3, 2)


def places():
    return lax.axis_index("kv_0"), lax.axis_index("kv_1"), lax.axis_index("tp")


def remote(src, dst, send_sem, recv_sem, **where):
    return pltpu.make_async_remote_copy(
        src_ref=src, dst_ref=dst, send_sem=send_sem, recv_sem=recv_sem,
        device_id=where, device_id_type=MESH_ID,
    )


def greet(z, y, c, with_tp):
    barrier = pltpu.get_barrier_semaphore()
    for d in range(1, NZ):
        pl.semaphore_signal(barrier, inc=1, device_id={"kv_0": (z + d) % NZ}, device_id_type=MESH_ID)
    for d in range(1, NY):
        pl.semaphore_signal(barrier, inc=1, device_id={"kv_1": (y + d) % NY}, device_id_type=MESH_ID)
    if with_tp:
        pl.semaphore_signal(barrier, inc=1, device_id={"tp": 1 - c}, device_id_type=MESH_ID)
    pl.semaphore_wait(barrier, NZ - 1 + NY - 1 + int(with_tp))


def gather_2d(buf, z, y, zs, zr, ys, yr):
    def z_copy(d):
        return remote(buf.at[z, y], buf.at[z, y], zs.at[d], zr.at[d], kv_0=(z + d) % NZ)

    def y_copy(k, e):
        row = (z + NZ - k) % NZ
        return remote(buf.at[row, y], buf.at[row, y], ys.at[k, e], yr.at[k, e], kv_1=(y + e) % NY)

    for d in Z_STEPS:
        z_copy(d).start()
    for e in Y_STEPS:
        y_copy(0, e).start()
    for d in Z_STEPS:
        z_copy(d).wait_recv()
        for e in Y_STEPS:
            y_copy(d, e).start()
    for d in Z_STEPS:
        z_copy(d).wait_send()
    for k in (0, *Z_STEPS):
        for e in Y_STEPS:
            y_copy(k, e).wait()


def project_kernel(tok, gain, wq, wk, wv, cs, sn, qg, kvb, tokg, gaing, wbuf, nrm, pq, pkv, zq, zkv,
                   ws, wr, ts, tr, gs, gr, ls, qs, qr, ks, kr, azs, azr, ays, ayr):
    z, y, c = places()
    gaing[y] = jnp.broadcast_to(gain[...], (16, 128))
    greet(z, y, c, False)
    ws_in = (wq, wk, wv)

    def tok_copy(e):
        return remote(tok, tokg.at[y], ts.at[e], tr.at[e], kv_1=(y + e) % NY)

    def gain_copy(e):
        return remote(gaing.at[y], gaing.at[y], gs.at[e], gr.at[e], kv_1=(y + e) % NY)

    def w_copy(m, e):
        to = (y + e) % NY
        cols = pl.ds(pl.multiple_of(to * 512, 512), 512)
        return remote(ws_in[m].at[:, cols], wbuf.at[m, y], ws.at[m, e], wr.at[m, e], kv_1=to)

    for e in Y_STEPS:
        gain_copy(e).start()
        tok_copy(e).start()
    for m in range(3):
        for e in Y_STEPS:
            w_copy(m, e).start()
    mine = pl.ds(pl.multiple_of(y * 512, 512), 512)
    own = [pltpu.make_async_copy(ws_in[m].at[:, mine], wbuf.at[m, y], ls.at[m]) for m in range(3)]
    for o in own:
        o.start()
    tokg[y] = tok[...]
    for e in Y_STEPS:
        gain_copy(e).wait_recv()
        tok_copy(e).wait_recv()
    power = jnp.zeros((256, 1), F32)
    for a in range(NY):
        wide = tokg[a].astype(F32)
        power += jnp.sum(wide * wide, axis=-1, keepdims=True)
        nrm[:, a * 128:(a + 1) * 128] = (wide * gaing[a, 0:1].astype(F32)).astype(BF16)
    high = power.astype(BF16)
    rest = power - high.astype(F32)
    mid = rest.astype(BF16)
    low = (rest - mid.astype(F32)).astype(BF16)
    lane = lax.broadcasted_iota(jnp.int32, (256, 128), 1)
    terms = jnp.where(lane == 0, high.astype(F32), jnp.where(lane == 1, mid.astype(F32), low.astype(F32)))
    terms = jnp.where(lane < 3, terms, 0.0)
    pq[:, :, 512:640] = terms.astype(BF16).reshape(NZ, 32, 128)

    def product(m):
        own[m].wait()
        for e in Y_STEPS:
            w_copy(m, e).wait_recv()
        out = jnp.zeros((256, 512), F32)
        for a in range(NY):
            out += jnp.dot(nrm[:, a * 128:(a + 1) * 128], wbuf[m, a], preferred_element_type=F32)
        return out.astype(BF16).reshape(NZ, 32, 512)

    def q_copy(d):
        to = (z + d) % NZ
        return remote(pq.at[to], zq.at[d], qs.at[d], qr.at[d], kv_0=to)

    def kv_copy(m, d):
        to = (z + d) % NZ
        return remote(pkv.at[m, to], zkv.at[m, d], ks.at[m, d], kr.at[m, d], kv_0=to)

    pq[:, :, 0:512] = product(0)
    for d in Z_STEPS:
        q_copy(d).start()
    for m in range(2):
        pkv[m] = product(m + 1)
        for d in Z_STEPS:
            kv_copy(m, d).start()

    total = pq[z].astype(F32)
    for d in Z_STEPS:
        q_copy(d).wait_recv()
        total += zq[d].astype(F32)
    power = jnp.sum(total[:, 512:640], axis=-1, keepdims=True)
    scale = lax.rsqrt(power / D + 1e-06)
    cos, sin = cs[...], sn[...]

    def turned(block):
        return block * cos + pltpu.roll(block, 64, 1) * sin

    for v in range(4):
        cols = slice(v * 128, (v + 1) * 128)
        turn = turned(total[:, cols] * scale).astype(BF16)
        qg[z, y, 0, :, cols] = turn[0:16]
        qg[z, y, 1, :, cols] = turn[16:32]
    gather_2d(qg, z, y, azs, azr, ays, ayr)

    for m in range(2):
        total = pkv[m, z].astype(F32)
        for d in Z_STEPS:
            kv_copy(m, d).wait_recv()
            total += zkv[m, d].astype(F32)
        for v in range(4):
            block = total[:, v * 128:(v + 1) * 128] * scale
            if m == 0:
                block = turned(block)
            at = m * 512 + v * 128
            kvb[:, at:at + 128] = block.astype(BF16)
    for e in Y_STEPS:
        gain_copy(e).wait_send()
        tok_copy(e).wait_send()
        for m in range(3):
            w_copy(m, e).wait_send()
    for d in Z_STEPS:
        q_copy(d).wait_send()
        for m in range(2):
            kv_copy(m, d).wait_send()


def vmem(n):
    return [pl.BlockSpec(memory_space=pltpu.VMEM)] * n


def project(tokens, gain, wq, wk, wv, cs, sn):
    return pl.pallas_call(
        project_kernel,
        name="project",
        out_shape=(
            jax.ShapeDtypeStruct((NZ, NY, 2, 16, 512), BF16),
            jax.ShapeDtypeStruct((32, 1024), BF16),
        ),
        in_specs=vmem(7),
        out_specs=tuple(vmem(2)),
        scratch_shapes=[
            pltpu.VMEM((NY, 256, 128), BF16),
            pltpu.VMEM((NY, 16, 128), BF16),
            pltpu.VMEM((3, NY, 128, 512), BF16),
            pltpu.VMEM((256, 512), BF16),
            pltpu.VMEM((NZ, 32, 640), BF16),
            pltpu.VMEM((2, NZ, 32, 512), BF16),
            pltpu.VMEM((NZ, 32, 640), BF16),
            pltpu.VMEM((2, NZ, 32, 512), BF16),
            DMA((3, NY)), DMA((3, NY)), DMA((NY,)), DMA((NY,)), DMA((NY,)), DMA((NY,)), DMA((3,)),
            DMA((NZ,)), DMA((NZ,)), DMA((2, NZ)), DMA((2, NZ)),
            DMA((NZ,)), DMA((NZ,)), DMA((NZ, NY)), DMA((NZ, NY)),
        ],
        compiler_params=pltpu.CompilerParams(collective_id=0, has_side_effects=True),
    )(tokens, gain, wq, wk, wv, cs, sn)


def contract(a, b, dims):
    return lax.dot_general(a, b, (dims, ((), ())), preferred_element_type=F32)


def attend_kernel(meta, q_ref, k_ref, v_ref, kv_ref, om_ref, st_ref, acc_ref, pick):
    b = pl.program_id(0)

    @pl.when(b == 0)
    def _():
        out_row = lax.broadcasted_iota(jnp.int32, (256, 256), 0)
        in_row = lax.broadcasted_iota(jnp.int32, (256, 256), 1)
        source = ((out_row % 128) // 8) * 16 + (out_row % 8) * 2 + out_row // 128
        pick[...] = (source == in_row).astype(F32).astype(BF16)

    limit, mine = meta[0, b], meta[1, b]
    halves = [
        jnp.dot(pick[...], k_ref[0, i * 256:(i + 1) * 256], preferred_element_type=F32).astype(BF16)
        for i in range(2)
    ]
    row = lax.broadcasted_iota(jnp.int32, (256, 128), 0)
    lane = lax.broadcasted_iota(jnp.int32, (256, 128), 1)
    live = ((row % 8) == (lane // 16)) & ((row // 8) < limit)
    live = jnp.concatenate([live.astype(F32), om_ref[0] * mine.astype(F32)], axis=0) > 0.5
    values = jnp.concatenate(
        [v_ref[0], kv_ref[0, :, 512:768], kv_ref[0, :, 768:1024]], axis=0
    )
    for m in range(2):
        keys = jnp.concatenate(
            [halves[i][m * 128:(m + 1) * 128] for i in range(2)]
            + [kv_ref[0, :, (h * 2 + m) * 128:(h * 2 + m + 1) * 128] for h in range(2)], axis=0
        )
        queries = jnp.concatenate(
            [q_ref[0, i, 0, :, (h * 2 + m) * 128:(h * 2 + m + 1) * 128] for i in range(NY) for h in range(2)], axis=0
        )
        s = contract(keys, queries, ((1,), (1,))) * ROOT
        s = jnp.where(live, s, NEG_FILL)
        peak = jnp.max(s, axis=0, keepdims=True)
        e = jnp.where(live, jnp.exp(s - peak), 0.0)
        st_ref[0, 0, m:m + 1] = peak
        st_ref[1, 0, m:m + 1] = jnp.sum(e, axis=0, keepdims=True)
        acc_ref[0, m * 128:(m + 1) * 128] = contract(e.astype(BF16), values, ((0,), (0,))).astype(BF16)


def attend(meta, queries, keys, values, own_kv, own_mask):
    return pl.pallas_call(
        attend_kernel,
        name="attend",
        grid_spec=pltpu.PrefetchScalarGridSpec(
            num_scalar_prefetch=1,
            grid=(16,),
            in_specs=[
                pl.BlockSpec((1, NY, 1, 16, 512), lambda b, meta: (b // 2, 0, b % 2, 0, 0)),
                pl.BlockSpec((1, 512, 128), lambda b, meta: (b, 0, 0)),
                pl.BlockSpec((1, 256, 256), lambda b, meta: (b, 0, 0)),
                pl.BlockSpec((1, 16, 1024), lambda b, meta: (b % 2, 0, 0)),
                pl.BlockSpec((1, 32, 128), lambda b, meta: (b % 2, 0, 0)),
            ],
            out_specs=(
                pl.BlockSpec((2, 1, 2, 128), lambda b, meta: (0, b, 0, 0)),
                pl.BlockSpec((1, 256, 256), lambda b, meta: (b, 0, 0)),
            ),
            scratch_shapes=[pltpu.VMEM((256, 256), BF16)],
        ),
        out_shape=(
            jax.ShapeDtypeStruct((2, 16, 2, 128), F32),
            jax.ShapeDtypeStruct((16, 256, 256), BF16),
        ),
    )(meta, queries, keys, values, own_kv.reshape(2, 16, 1024), own_mask)


def merged(parts):
    peak = functools.reduce(jnp.maximum, [p for p, _ in parts])
    total = sum(t * jnp.exp(p - peak) for p, t in parts)
    return peak, total


def finish_kernel(st, acc, lam, sub, wo, out, yst, ysum, zst, gst, bs, ybuf, zsum, zbuf, mg, prod, got,
                  ss, sr, s2, r2, s3, r3, bss, bsr, zs, zr, azs, azr, ays, ayr, cs, cr):
    z, y, c = places()
    greet(z, y, c, True)

    def st_copy(e):
        return remote(st, yst.at[e], ss.at[e], sr.at[e], kv_1=(y + e) % NY)

    for e in Y_STEPS:
        st_copy(e).start()
    parts = [(st[:, 0], st[:, 1])]
    for e in Y_STEPS:
        st_copy(e).wait_recv()
        parts.append((yst[e, :, 0], yst[e, :, 1]))
    peak, total = merged(parts)
    ysum[:, 0] = peak
    ysum[:, 1] = total

    def st_z(d):
        to = (z + d) % NZ
        return remote(ysum.at[to], zst.at[d], s2.at[d], r2.at[d], kv_0=to)

    for d in Z_STEPS:
        st_z(d).start()
    parts = [(ysum[z, 0], ysum[z, 1])]
    for d in Z_STEPS:
        st_z(d).wait_recv()
        parts.append((zst[d, 0], zst[d, 1]))
    peak, total = merged(parts)
    gst[z, 0] = peak
    gst[z, 1] = 1.0 / total

    def g_copy(d):
        return remote(gst.at[z], gst.at[z], s3.at[d], r3.at[d], kv_0=(z + d) % NZ)

    for d in Z_STEPS:
        g_copy(d).start()
    for d in Z_STEPS:
        g_copy(d).wait_recv()

    row = lax.broadcasted_iota(jnp.int32, (128, 128), 0)
    lane = lax.broadcasted_iota(jnp.int32, (128, 128), 1)
    same = row == lane

    def b_copy(zc, e):
        to = (y + e) % NY
        return remote(bs.at[to, zc], ybuf.at[e, zc], bss.at[zc, e], bsr.at[zc, e], kv_1=to)

    def send_z(d):
        to = (z + d) % NZ
        return remote(zsum.at[to], zbuf.at[d], zs.at[d], zr.at[d], kv_0=to)

    def blocks(d, carry):
        zc = (z + d) % NZ
        ratio = jnp.exp(st[zc, 0] - gst[zc, 0]) * gst[zc, 1]
        for s in range(2):
            first = jnp.where(same, ratio[2 * s:2 * s + 1], 0.0)
            second = jnp.where(same, ratio[2 * s + 1:2 * s + 2] * -lam[...], 0.0)
            mix = jnp.concatenate([first, second], axis=1).astype(BF16)
            block = jnp.dot(mix, acc[zc, s], preferred_element_type=F32).astype(BF16)
            for i in range(NY):
                bs[i, zc, s] = block[i * 32:(i + 1) * 32]
        for e in Y_STEPS:
            b_copy(zc, e).start()
        return carry

    lax.fori_loop(1, NZ + 1, blocks, 0)

    def sums(d, carry):
        zc = (z + d) % NZ
        total = bs[y, zc].astype(F32)
        for e in Y_STEPS:
            b_copy(zc, e).wait_recv()
            total += ybuf[e, zc].astype(F32)
        zsum[zc] = total.astype(BF16)

        @pl.when(d < NZ)
        def _():
            send_z(d).start()

        return carry

    lax.fori_loop(1, NZ + 1, sums, 0)
    total = zsum[z].astype(F32)
    for d in range(1, NZ):
        send_z(d).wait_recv()
        total += zbuf[d].astype(F32)
    norm = total * lax.rsqrt(jnp.mean(total * total, axis=-1, keepdims=True) + 1e-05)
    mg[z, y] = (norm * sub[...] * LAMBDA_SCALE).astype(BF16)
    gather_2d(mg, z, y, azs, azr, ays, ayr)
    product = jnp.zeros((256, 128), F32)
    for h in range(8):
        i, k = h // 2, h % 2
        rows = jnp.concatenate(
            [mg[a, i, s, k * 16:(k + 1) * 16] for a in range(NZ) for s in range(2)], axis=0
        )
        product += jnp.dot(rows, wo[h * 256:(h + 1) * 256], preferred_element_type=F32)
    prod[...] = product.astype(BF16)
    swap = remote(prod, got, cs, cr, tp=1 - c)
    swap.start()
    swap.wait()
    result = (prod[...].astype(F32) + got[...].astype(F32)).astype(BF16)
    out[...] = jnp.where(c == 0, result[:, 0:64].astype(F32), result[:, 64:128].astype(F32)).astype(BF16)

    for e in Y_STEPS:
        st_copy(e).wait_send()
    for d in Z_STEPS:
        st_z(d).wait_send()
        g_copy(d).wait_send()
        send_z(d).wait_send()

    def drain(zc, carry):
        for e in Y_STEPS:
            b_copy(zc, e).wait_send()
        return carry

    lax.fori_loop(0, NZ, drain, 0)


def finish(stats, acc, lam, sub, wo):
    return pl.pallas_call(
        finish_kernel,
        name="finish",
        out_shape=jax.ShapeDtypeStruct((256, 64), BF16),
        in_specs=vmem(5),
        out_specs=vmem(1)[0],
        scratch_shapes=[
            pltpu.VMEM((NY, NZ, 2, 4, 128), F32),
            pltpu.VMEM((NZ, 2, 4, 128), F32),
            pltpu.VMEM((NZ, 2, 4, 128), F32),
            pltpu.VMEM((NZ, 2, 4, 128), F32),
            pltpu.VMEM((NY, NZ, 2, 32, 256), BF16),
            pltpu.VMEM((NY, NZ, 2, 32, 256), BF16),
            pltpu.VMEM((NZ, 2, 32, 256), BF16),
            pltpu.VMEM((NZ, 2, 32, 256), BF16),
            pltpu.VMEM((NZ, NY, 2, 32, 256), BF16),
            pltpu.VMEM((256, 128), BF16),
            pltpu.VMEM((256, 128), BF16),
            DMA((NY,)), DMA((NY,)), DMA((NZ,)), DMA((NZ,)), DMA((NZ,)), DMA((NZ,)),
            DMA((NZ, NY)), DMA((NZ, NY)), DMA((NZ,)), DMA((NZ,)),
            DMA((NZ,)), DMA((NZ,)), DMA((NZ, NY)), DMA((NZ, NY)), DMA, DMA,
        ],
        compiler_params=pltpu.CompilerParams(collective_id=1, has_side_effects=True),
    )(stats, acc, lam, sub, wo)


def spread_kernel(kvb, kvg, zs, zr, ys, yr, ls):
    z, y, c = places()
    greet(z, y, c, False)
    upper = z >= NZ // 2

    def z_copy(d):
        return remote(kvb, kvg.at[z, y], zs.at[d], zr.at[d], kv_0=(z + d) % NZ)

    def z_in(d):
        return (z + NZ - d) % NZ

    def y_copy(k, e):
        row = (z + NZ - k) % NZ
        return remote(kvg.at[row, y], kvg.at[row, y], ys.at[k, e], yr.at[k, e], kv_1=(y + e) % NY)

    for d in Z_STEPS:
        @pl.when((z + d) % NZ >= NZ // 2)
        def _():
            z_copy(d).start()

    @pl.when(upper)
    def _():
        own = pltpu.make_async_copy(kvb, kvg.at[z, y], ls)
        own.start()
        own.wait()
        for e in Y_STEPS:
            y_copy(0, e).start()
        for d in Z_STEPS:
            z_copy(d).wait_recv()
            for e in Y_STEPS:
                y_copy(d, e).start()
        for k in (0, *Z_STEPS):
            for e in Y_STEPS:
                y_copy(k, e).wait()

    for d in Z_STEPS:
        @pl.when((z + d) % NZ >= NZ // 2)
        def _():
            z_copy(d).wait_send()


def spread(kvb):
    return pl.pallas_call(
        spread_kernel,
        name="spread",
        out_shape=jax.ShapeDtypeStruct((NZ, NY, 32, 1024), BF16),
        in_specs=vmem(1),
        out_specs=vmem(1)[0],
        scratch_shapes=[DMA((NZ,)), DMA((NZ,)), DMA((NZ, NY)), DMA((NZ, NY)), DMA],
        compiler_params=pltpu.CompilerParams(collective_id=2, has_side_effects=True),
    )(kvb)


def insert_kernel(slot, k_ref, v_ref, nk_ref, nv_ref, ko_ref, vo_ref, kt, vt):
    at = slot[pl.program_id(0)]
    kt[16:48] = k_ref[0]
    vt[16:48] = v_ref[0]
    kt[pl.ds(at, 16)] = nk_ref[0]
    vt[pl.ds(at, 16)] = nv_ref[0]
    ko_ref[0] = kt[16:48]
    vo_ref[0] = vt[16:48]


def insert(slot, keys, values, new_keys, new_values):
    def spec(*shape):
        return pl.BlockSpec((1, *shape), lambda b, slot: (b, 0, 0, 0))

    return pl.pallas_call(
        insert_kernel,
        name="insert",
        grid_spec=pltpu.PrefetchScalarGridSpec(
            num_scalar_prefetch=1,
            grid=(16,),
            in_specs=[spec(32, 16, 128), spec(32, 8, 256), spec(16, 16, 128), spec(16, 8, 256)],
            out_specs=(spec(32, 16, 128), spec(32, 8, 256)),
            scratch_shapes=[pltpu.VMEM((64, 16, 128), BF16), pltpu.VMEM((64, 8, 256), BF16)],
        ),
        out_shape=(
            jax.ShapeDtypeStruct((16, 32, 16, 128), BF16),
            jax.ShapeDtypeStruct((16, 32, 8, 256), BF16),
        ),
    )(slot, keys, values, new_keys, new_values)


def per_device(tokens, in_gain, query_weight, key_weight, value_weight, out_weight, lambdas, sub_gain,
               key_cache, value_cache, cache_len, accepted, parents):
    z, y = lax.axis_index("kv_0"), lax.axis_index("kv_1")
    starts = cache_len + accepted
    offset = (z * NY + y) * 32

    near = lax.dynamic_slice_in_dim(parents, 2 * z, 2, 0)
    number = jnp.arange(16, dtype=jnp.int32)
    reach = jnp.maximum(
        jnp.eye(16, dtype=F32)[None], (near[:, :, None] == number[None, None, :]).astype(F32)
    )
    for _ in range(4):
        reach = jnp.max(reach[:, :, :, None] * reach[:, None, :, :], axis=2)
    depth = (jnp.sum(reach, axis=-1) - 1.0).astype(jnp.int32)
    position = (lax.dynamic_slice_in_dim(starts, 2 * z, 2, 0)[:, None] + depth).reshape(32)
    frequency = 10000.0 ** (-jnp.arange(64, dtype=F32) / 64)
    angles = position.astype(F32)[:, None] * frequency[None, :]
    cosine, sine = jnp.cos(angles), jnp.sin(angles)
    cs = jnp.concatenate([cosine, cosine], axis=1)
    sn = jnp.concatenate([-sine, sine], axis=1)

    head_row = 2 * y + jnp.arange(32) // 16
    head_lane = jnp.arange(128) // 16
    seen = jnp.tile(reach.transpose(0, 2, 1), (1, 2, 8))
    own_mask = jnp.where(head_row[:, None] == head_lane[None, :], seen, 0.0)
    meta = jnp.stack([starts - offset, (jnp.arange(16) // 2 == z).astype(jnp.int32)])

    queries, own_kv = project(
        tokens.reshape(256, 128), in_gain.reshape(1, 128), query_weight, key_weight, value_weight, cs, sn
    )
    stats, acc = attend(
        meta, queries, key_cache.reshape(16, 512, 128), value_cache.reshape(16, 256, 256), own_kv, own_mask
    )
    lam = jnp.repeat(lambdas, 16)[None, :]
    stats = stats.reshape(2, NZ, 4, 128).transpose(1, 0, 2, 3)
    output = finish(
        stats, acc.reshape(NZ, 2, 256, 256), lam, sub_gain.astype(F32).reshape(1, 256), out_weight
    )
    both = spread(own_kv).reshape(NZ, NY, 2, 16, 1024).transpose(0, 2, 3, 1, 4)
    new_keys = both[..., :512].reshape(16, 16, 16, 128)
    new_values = both[..., 512:].reshape(16, 16, 8, 256)
    slot = jnp.clip(starts - offset + 16, 0, 48)
    key_out, value_out = insert(slot, key_cache.reshape(16, 32, 16, 128), value_cache, new_keys, new_values)
    return output.reshape(16, 16, 64), key_out.reshape(key_cache.shape), value_out


def solution(mesh):
    torus = Mesh(mesh.devices.reshape(mesh.shape["dp"], NZ, NY, mesh.shape["tp"]), ("dp", "kv_0", "kv_1", "tp"))
    placed = (
        P("dp", None, KV), P(KV), P(KV, "tp"), P(KV, "tp"), P(KV, "tp"), P("tp", KV), P("tp"), P(),
        P("dp", KV, "tp", None, None), P("dp", KV, "tp", None), P("dp"), P("dp"), P("dp", None),
    )
    return jax.shard_map(
        per_device, mesh=torus, in_specs=placed,
        out_specs=(P("dp", None, KV_TP), P("dp", KV, "tp", None, None), P("dp", KV, "tp", None)),
        check_vma=False,
    )
```

```python
import functools
import math

import jax
import jax.numpy as jnp
import numpy as np
from jax import lax
from jax.experimental import pallas as pl
from jax.experimental.pallas import tpu as pltpu
from jax.sharding import Mesh
from jax.sharding import PartitionSpec as P

D = 4096
NZ, NY = 8, 4
KV = ("kv_0", "kv_1")
KV_TP = ("kv_0", "kv_1", "tp")
LAMBDA_SCALE = 0.2 + 0.6 * math.exp(-0.6)
NEG_FILL = -1e30
ROOT = 128 ** (-0.5)
F32, BF16 = jnp.float32, jnp.bfloat16
MESH_ID = pl.DeviceIdType.MESH
DMA = pltpu.SemaphoreType.DMA
Z_STEPS = (1, 7, 2, 6, 3, 5, 4)
Y_STEPS = (1, 3, 2)


def places():
    return lax.axis_index("kv_0"), lax.axis_index("kv_1"), lax.axis_index("tp")


def remote(src, dst, send_sem, recv_sem, **where):
    return pltpu.make_async_remote_copy(
        src_ref=src, dst_ref=dst, send_sem=send_sem, recv_sem=recv_sem,
        device_id=where, device_id_type=MESH_ID,
    )


def greet(z, y, c, with_tp):
    barrier = pltpu.get_barrier_semaphore()
    for d in range(1, NZ):
        pl.semaphore_signal(barrier, inc=1, device_id={"kv_0": (z + d) % NZ}, device_id_type=MESH_ID)
    for d in range(1, NY):
        pl.semaphore_signal(barrier, inc=1, device_id={"kv_1": (y + d) % NY}, device_id_type=MESH_ID)
    if with_tp:
        pl.semaphore_signal(barrier, inc=1, device_id={"tp": 1 - c}, device_id_type=MESH_ID)
    pl.semaphore_wait(barrier, NZ - 1 + NY - 1 + int(with_tp))


def gather_2d(buf, z, y, zs, zr, ys, yr):
    def z_copy(d):
        return remote(buf.at[z, y], buf.at[z, y], zs.at[d], zr.at[d], kv_0=(z + d) % NZ)

    def y_copy(k, e):
        row = (z + NZ - k) % NZ
        return remote(buf.at[row, y], buf.at[row, y], ys.at[k, e - 1], yr.at[k, e - 1], kv_1=(y + e) % NY)

    def start():
        for d in Z_STEPS:
            z_copy(d).start()
        for e in Y_STEPS:
            y_copy(0, e).start()

    def hand_on():
        for d in Z_STEPS:
            z_copy(d).wait_recv()
            for e in Y_STEPS:
                y_copy(d, e).start()

    def end():
        for d in Z_STEPS:
            z_copy(d).wait_send()
        for k in (0, *Z_STEPS):
            for e in Y_STEPS:
                y_copy(k, e).wait()

    return start, hand_on, end


def contract(a, b, dims):
    return lax.dot_general(a, b, (dims, ((), ())), preferred_element_type=F32)


def merged(parts):
    peak = functools.reduce(jnp.maximum, [p for p, _ in parts])
    total = sum(t * jnp.exp(p - peak) for p, t in parts)
    return peak, total


def layer_kernel(length, accepted, lambdas, parents, tok, gain, sub, freq, wq, wk, wv, keys_in, values_in, wo_in,
                 out, kvg,
                 tokg, gaing, wbuf, nrm, pq, pkv, zq, zkv, qg, kvown, kc, vc, wo, code, pscr, st, sx, mst, acc, accx,
                 yst, ysum, zst, gst, bs, ybuf, zsum, zbuf, mg, prod, got,
                 ls, ws, wr, ts, tr, gs, gr, qs, qr, ks, kr, azs, azr, ays, ayr, kzs, kzr, kys, kyr,
                 ss, sr, s2, r2, s3, r3, bss, bsr, zs, zr, xs, xr):
    z, y, c = places()
    loads = [
        pltpu.make_async_copy(src, dst, ls.at[3 + i])
        for i, (src, dst) in enumerate(((keys_in, kc), (values_in, vc), (wo_in, wo)))
    ]
    gaing[y] = jnp.broadcast_to(gain[...], (16, 128))
    greet(z, y, c, True)
    ws_in = (wq, wk, wv)

    def tok_copy(e):
        return remote(tok, tokg.at[y], ts.at[e], tr.at[e], kv_1=(y + e) % NY)

    def gain_copy(e):
        return remote(gaing.at[y], gaing.at[y], gs.at[e], gr.at[e], kv_1=(y + e) % NY)

    def w_copy(m, e):
        to = (y + e) % NY
        cols = pl.ds(pl.multiple_of(to * 512, 512), 512)
        return remote(ws_in[m].at[:, cols], wbuf.at[m, y], ws.at[m, e], wr.at[m, e], kv_1=to)

    for e in Y_STEPS:
        gain_copy(e).start()
        tok_copy(e).start()
    for m in range(3):
        for e in Y_STEPS:
            w_copy(m, e).start()
    mine = pl.ds(pl.multiple_of(y * 512, 512), 512)
    own = [pltpu.make_async_copy(ws_in[m].at[:, mine], wbuf.at[m, y], ls.at[m]) for m in range(3)]
    for o in own:
        o.start()
    for load in loads:
        load.start()
    tokg[y] = tok[...]

    row16 = lax.broadcasted_iota(jnp.int32, (16, 16), 0)
    lane16 = lax.broadcasted_iota(jnp.int32, (16, 16), 1)
    unit = (row16 == lane16).astype(F32)
    spread16 = (lax.broadcasted_iota(jnp.int32, (16, 128), 1) % 16 == lax.broadcasted_iota(jnp.int32, (16, 128), 0)).astype(BF16)
    near = parents[pl.ds(2 * z, 2), :]
    seen, angles = [], []
    for s in range(2):
        reach = jnp.maximum(unit, (near[s:s + 1, :] == row16).astype(F32))
        for _ in range(4):
            half = reach.astype(BF16)
            reach = jnp.minimum(jnp.dot(half, half, preferred_element_type=F32), 1.0)
        half = reach.astype(BF16)
        seen.append(jnp.dot(half, spread16, preferred_element_type=F32))
        depth = contract(half, jnp.ones((16, 128), BF16), ((0,), (0,))) - 1.0
        begin = length[2 * z + s] + accepted[2 * z + s]
        angles.append((begin.astype(F32) + depth) * freq[...])
    angle = jnp.concatenate(angles, axis=0)
    cos = jnp.cos(angle)
    sin = jnp.where(lax.broadcasted_iota(jnp.int32, (32, 128), 1) < 64, -1.0, 1.0) * jnp.sin(angle)
    row = lax.broadcasted_iota(jnp.int32, (512, 128), 0)
    lane = lax.broadcasted_iota(jnp.int32, (512, 128), 1)
    code[...] = jnp.where(((row // 2) % 8) == (lane // 16), row // 16, 4096)

    for e in Y_STEPS:
        gain_copy(e).wait_recv()
        tok_copy(e).wait_recv()
    power = jnp.zeros((256, 1), F32)
    for a in range(NY):
        wide = tokg[a].astype(F32)
        power += jnp.sum(wide * wide, axis=-1, keepdims=True)
        nrm[:, a * 128:(a + 1) * 128] = (wide * gaing[a, 0:1].astype(F32)).astype(BF16)
    high = power.astype(BF16)
    rest = power - high.astype(F32)
    mid = rest.astype(BF16)
    low = (rest - mid.astype(F32)).astype(BF16)
    lane = lax.broadcasted_iota(jnp.int32, (256, 128), 1)
    terms = jnp.where(lane == 0, high.astype(F32), jnp.where(lane == 1, mid.astype(F32), low.astype(F32)))
    terms = jnp.where(lane < 3, terms, 0.0)
    pq[:, :, 512:640] = terms.astype(BF16).reshape(NZ, 32, 128)

    def product(m):
        own[m].wait()
        for e in Y_STEPS:
            w_copy(m, e).wait_recv()
        total = jnp.zeros((256, 512), F32)
        for a in range(NY):
            total += jnp.dot(nrm[:, a * 128:(a + 1) * 128], wbuf[m, a], preferred_element_type=F32)
        return total.astype(BF16).reshape(NZ, 32, 512)

    def q_copy(d):
        to = (z + d) % NZ
        return remote(pq.at[to], zq.at[d], qs.at[d], qr.at[d], kv_0=to)

    def kv_copy(m, d):
        to = (z + d) % NZ
        return remote(pkv.at[m, to], zkv.at[m, d], ks.at[m, d], kr.at[m, d], kv_0=to)

    pq[:, :, 0:512] = product(0)
    for d in Z_STEPS:
        q_copy(d).start()
    pkv[0] = product(1)
    for d in Z_STEPS:
        kv_copy(0, d).start()

    total = pq[z].astype(F32)
    for d in Z_STEPS:
        q_copy(d).wait_recv()
        total += zq[d].astype(F32)
    power = jnp.sum(total[:, 512:640], axis=-1, keepdims=True)
    scale = lax.rsqrt(power / D + 1e-06)

    def turned(block):
        return block * cos + pltpu.roll(block, 64, 1) * sin

    for v in range(4):
        cols = slice(v * 128, (v + 1) * 128)
        turn = turned(total[:, cols] * scale).astype(BF16)
        qg[z, y, 0, :, cols] = turn[0:16]
        qg[z, y, 1, :, cols] = turn[16:32]
    q_start, q_hand_on, q_end = gather_2d(qg, z, y, azs, azr, ays, ayr)
    q_start()
    pkv[1] = product(2)
    for d in Z_STEPS:
        kv_copy(1, d).start()
    q_hand_on()

    for m in range(2):
        total = pkv[m, z].astype(F32)
        for d in Z_STEPS:
            kv_copy(m, d).wait_recv()
            total += zkv[m, d].astype(F32)
        for v in range(4):
            block = total[:, v * 128:(v + 1) * 128] * scale
            if m == 0:
                block = turned(block)
            at = m * 512 + v * 128
            kvown[:, at:at + 128] = block.astype(BF16)

    upper = z >= NZ // 2

    def up_z(d):
        return remote(kvown, kvg.at[z, y], kzs.at[d], kzr.at[d], kv_0=(z + d) % NZ)

    def up_y(k, e):
        at = (z + NZ - k) % NZ
        return remote(kvg.at[at, y], kvg.at[at, y], kys.at[k, e - 1], kyr.at[k, e - 1], kv_1=(y + e) % NY)

    own_up = pltpu.make_async_copy(kvown, kvg.at[z, y], ls.at[6])

    def to_upper(d, act):
        @pl.when((z + d) % NZ >= NZ // 2)
        def _():
            act(up_z(d))

    def hand_up(steps):
        @pl.when(upper)
        def _():
            for k in steps:
                if k == 0:
                    own_up.wait()
                else:
                    up_z(k).wait_recv()
                for e in Y_STEPS:
                    up_y(k, e).start()

    for d in Z_STEPS:
        to_upper(d, lambda copy: copy.start())

    @pl.when(upper)
    def _():
        own_up.start()

    q_end()
    loads[0].wait()
    loads[1].wait()

    def queries_of(zc, s):
        return jnp.concatenate(
            [qg[zc, i, s, :, (h * 2 + m) * 128:(h * 2 + m + 1) * 128] for m in range(2) for i in range(NY) for h in range(2)],
            axis=0,
        )

    odd = lax.broadcasted_iota(jnp.int32, (8, 128), 0) % 2 == 1
    offset = (z * NY + y) * 32

    def attend(zc, carry):
        for s in range(2):
            b = 2 * zc + s
            limit = length[b] + accepted[b] - offset
            both = contract(kc[b], queries_of(zc, s), ((1,), (1,)))
            both = both.reshape(64, 8, 256)
            live = (code[...] < limit).reshape(64, 8, 128)
            score = jnp.where(odd[None], both[:, :, 128:], both[:, :, :128]) * ROOT
            score = jnp.where(live, score, NEG_FILL)
            top = jnp.max(score, axis=0)
            peaks = [jnp.max(jnp.where(odd == bool(m), top, NEG_FILL), axis=0, keepdims=True) for m in range(2)]
            peak = jnp.where(odd, peaks[1], peaks[0])
            grown = jnp.where(live, jnp.exp(score - peak[None]), 0.0)
            part = jnp.sum(grown, axis=0)
            for m in range(2):
                st[0, zc, 2 * s + m:2 * s + m + 1] = peaks[m]
                st[1, zc, 2 * s + m:2 * s + m + 1] = jnp.sum(jnp.where(odd == bool(m), part, 0.0), axis=0, keepdims=True)
            pscr[s] = grown.reshape(512, 128)
            chance = jnp.concatenate([pscr[s, pl.ds(m, 256, stride=2), :] for m in range(2)], axis=1).astype(BF16)
            acc[zc, s] = contract(chance, vc[b], ((0,), (0,))).astype(BF16)
        return carry

    lax.fori_loop(0, NZ, attend, 0)

    head_row = 2 * y + lax.broadcasted_iota(jnp.int32, (32, 128), 0) // 16
    head_lane = lax.broadcasted_iota(jnp.int32, (32, 128), 1) // 16
    for s in range(2):
        rows = slice(s * 16, (s + 1) * 16)
        keys = jnp.concatenate(
            [kvown[rows, (h * 2 + m) * 128:(h * 2 + m + 1) * 128] for m in range(2) for h in range(2)], axis=0
        )
        values = jnp.concatenate([kvown[rows, 512:768], kvown[rows, 768:1024]], axis=0)
        both = contract(keys, queries_of(z, s), ((1,), (1,)))
        live = (head_row == head_lane) & (jnp.concatenate([seen[s], seen[s]], axis=0) > 0.5)
        chance = []
        for m in range(2):
            score = jnp.where(live, both[m * 32:(m + 1) * 32, m * 128:(m + 1) * 128] * ROOT, NEG_FILL)
            peak = jnp.max(score, axis=0, keepdims=True)
            grown = jnp.where(live, jnp.exp(score - peak), 0.0)
            sx[0, 2 * s + m:2 * s + m + 1] = peak
            sx[1, 2 * s + m:2 * s + m + 1] = jnp.sum(grown, axis=0, keepdims=True)
            chance.append(grown)
        accx[s] = contract(jnp.concatenate(chance, axis=1).astype(BF16), values, ((0,), (0,))).astype(BF16)
    mst[...] = st[...]
    peak, total = merged([(st[0, z], st[1, z]), (sx[0], sx[1])])
    mst[0, z] = peak
    mst[1, z] = total

    def st_copy(e):
        return remote(mst, yst.at[e], ss.at[e], sr.at[e], kv_1=(y + e) % NY)

    for e in Y_STEPS:
        st_copy(e).start()
    parts = [(mst[0], mst[1])]
    for e in Y_STEPS:
        st_copy(e).wait_recv()
        parts.append((yst[e, 0], yst[e, 1]))
    peak, total = merged(parts)
    ysum[:, 0] = peak
    ysum[:, 1] = total

    def st_z(d):
        to = (z + d) % NZ
        return remote(ysum.at[to], zst.at[d], s2.at[d], r2.at[d], kv_0=to)

    for d in Z_STEPS:
        st_z(d).start()
    hand_up((0, 1, 7, 2))
    parts = [(ysum[z, 0], ysum[z, 1])]
    for d in Z_STEPS:
        st_z(d).wait_recv()
        parts.append((zst[d, 0], zst[d, 1]))
    peak, total = merged(parts)
    gst[z, 0] = peak
    gst[z, 1] = 1.0 / total

    def g_copy(d):
        return remote(gst.at[z], gst.at[z], s3.at[d], r3.at[d], kv_0=(z + d) % NZ)

    for d in Z_STEPS:
        g_copy(d).start()
    row = lax.broadcasted_iota(jnp.int32, (128, 128), 0)
    lane = lax.broadcasted_iota(jnp.int32, (128, 128), 1)
    same = row == lane
    lane = lax.broadcasted_iota(jnp.int32, (1, 128), 1) // 16
    lam = jnp.zeros((1, 128), F32)
    for h in range(8):
        lam = jnp.where(lane == h, -lambdas[h], lam)
    for d in Z_STEPS:
        g_copy(d).wait_recv()

    def b_copy(zc, e):
        to = (y + e) % NY
        return remote(bs.at[to, zc], ybuf.at[e - 1, zc], bss.at[zc, e - 1], bsr.at[zc, e - 1], kv_1=to)

    def send_z(d):
        to = (z + d) % NZ
        return remote(zsum.at[to], zbuf.at[d], zs.at[d], zr.at[d], kv_0=to)

    def mixing(peaks, zc, s):
        ratio = jnp.exp(peaks - gst[zc, 0]) * gst[zc, 1]
        first = jnp.where(same, ratio[2 * s:2 * s + 1], 0.0)
        second = jnp.where(same, ratio[2 * s + 1:2 * s + 2] * lam, 0.0)
        return jnp.concatenate([first, second], axis=1).astype(BF16)

    def send_blocks(zc, last):
        for s in range(2):
            block = jnp.dot(mixing(st[0, zc], zc, s), acc[zc, s], preferred_element_type=F32)
            if last:
                block += jnp.dot(mixing(sx[0], zc, s), accx[s], preferred_element_type=F32)
            block = block.astype(BF16)
            for i in range(NY):
                bs[i, zc, s] = block[i * 32:(i + 1) * 32]
        for e in Y_STEPS:
            b_copy(zc, e).start()

    def blocks(d, carry):
        send_blocks((z + d) % NZ, False)
        return carry

    lax.fori_loop(1, NZ, blocks, 0)
    send_blocks(z, True)
    hand_up((6, 3, 5, 4))

    def sums(d, carry):
        zc = (z + d) % NZ
        total = bs[y, zc].astype(F32)
        for e in Y_STEPS:
            b_copy(zc, e).wait_recv()
            total += ybuf[e - 1, zc].astype(F32)
        zsum[zc] = total.astype(BF16)

        @pl.when(d < NZ)
        def _():
            send_z(d).start()

        return carry

    lax.fori_loop(1, NZ + 1, sums, 0)
    total = zsum[z].astype(F32)
    for d in range(1, NZ):
        send_z(d).wait_recv()
        total += zbuf[d].astype(F32)
    norm = total * lax.rsqrt(jnp.mean(total * total, axis=-1, keepdims=True) + 1e-05)
    mg[z, y] = (norm * sub[...].astype(F32) * LAMBDA_SCALE).astype(BF16)
    m_start, m_hand_on, m_end = gather_2d(mg, z, y, azs, azr, ays, ayr)
    m_start()
    m_hand_on()
    loads[2].wait()
    m_end()
    result = jnp.zeros((256, 128), F32)
    for h in range(8):
        i, k = h // 2, h % 2
        rows = jnp.concatenate(
            [mg[a, i, s, k * 16:(k + 1) * 16] for a in range(NZ) for s in range(2)], axis=0
        )
        result += jnp.dot(rows, wo[h * 256:(h + 1) * 256], preferred_element_type=F32)
    prod[...] = result.astype(BF16)
    swap = remote(prod, got, xs, xr, tp=1 - c)
    swap.start()
    swap.wait()
    result = prod[...].astype(F32) + got[...].astype(F32)
    out[...] = jnp.where(c == 0, result[:, 0:64], result[:, 64:128]).astype(BF16)

    for e in Y_STEPS:
        gain_copy(e).wait_send()
        tok_copy(e).wait_send()
        st_copy(e).wait_send()
        for m in range(3):
            w_copy(m, e).wait_send()
    for d in Z_STEPS:
        q_copy(d).wait_send()
        for m in range(2):
            kv_copy(m, d).wait_send()
        st_z(d).wait_send()
        g_copy(d).wait_send()
        send_z(d).wait_send()
        to_upper(d, lambda copy: copy.wait_send())

    def drain(zc, carry):
        for e in Y_STEPS:
            b_copy(zc, e).wait_send()
        return carry

    lax.fori_loop(0, NZ, drain, 0)

    @pl.when(upper)
    def _():
        for k in (0, *Z_STEPS):
            for e in Y_STEPS:
                up_y(k, e).wait()


def layer(*operands):
    vmem, smem = pl.BlockSpec(memory_space=pltpu.VMEM), pl.BlockSpec(memory_space=pltpu.SMEM)
    anywhere = pl.BlockSpec(memory_space=pl.ANY)
    y_pair, z_pair = [DMA((NY,))] * 2, [DMA((NZ,))] * 2
    zy_pair = [DMA((NZ, NY - 1))] * 2
    return pl.pallas_call(
        layer_kernel,
        name="layer",
        out_shape=(
            jax.ShapeDtypeStruct((256, 64), BF16),
            jax.ShapeDtypeStruct((NZ, NY, 32, 1024), BF16),
        ),
        in_specs=[smem] * 3 + [vmem] * 8 + [anywhere] * 3,
        out_specs=(vmem, anywhere),
        scratch_shapes=[
            pltpu.VMEM((NY, 256, 128), BF16),
            pltpu.VMEM((NY, 16, 128), BF16),
            pltpu.VMEM((3, NY, 128, 512), BF16),
            pltpu.VMEM((256, 512), BF16),
            pltpu.VMEM((NZ, 32, 640), BF16),
            pltpu.VMEM((2, NZ, 32, 512), BF16),
            pltpu.VMEM((NZ, 32, 640), BF16),
            pltpu.VMEM((2, NZ, 32, 512), BF16),
            pltpu.VMEM((NZ, NY, 2, 16, 512), BF16),
            pltpu.VMEM((32, 1024), BF16),
            pltpu.VMEM((16, 512, 128), BF16),
            pltpu.VMEM((16, 256, 256), BF16),
            pltpu.VMEM((2048, 128), BF16),
            pltpu.VMEM((512, 128), jnp.int32),
            pltpu.VMEM((2, 512, 128), F32),
            pltpu.VMEM((2, NZ, 4, 128), F32),
            pltpu.VMEM((2, 4, 128), F32),
            pltpu.VMEM((2, NZ, 4, 128), F32),
            pltpu.VMEM((NZ, 2, 256, 256), BF16),
            pltpu.VMEM((2, 256, 256), BF16),
            pltpu.VMEM((NY, 2, NZ, 4, 128), F32),
            pltpu.VMEM((NZ, 2, 4, 128), F32),
            pltpu.VMEM((NZ, 2, 4, 128), F32),
            pltpu.VMEM((NZ, 2, 4, 128), F32),
            pltpu.VMEM((NY, NZ, 2, 32, 256), BF16),
            pltpu.VMEM((NY - 1, NZ, 2, 32, 256), BF16),
            pltpu.VMEM((NZ, 2, 32, 256), BF16),
            pltpu.VMEM((NZ, 2, 32, 256), BF16),
            pltpu.VMEM((NZ, NY, 2, 32, 256), BF16),
            pltpu.VMEM((256, 128), BF16),
            pltpu.VMEM((256, 128), BF16),
            DMA((7,)), DMA((3, NY)), DMA((3, NY)), *y_pair, *y_pair,
            *z_pair, DMA((2, NZ)), DMA((2, NZ)),
            *z_pair, *zy_pair, *z_pair, *zy_pair,
            *y_pair, *z_pair, *z_pair, *zy_pair, *z_pair, DMA, DMA,
        ],
        compiler_params=pltpu.CompilerParams(
            collective_id=0, has_side_effects=True, vmem_limit_bytes=56 * 1024 * 1024
        ),
    )(*operands)


def insert_kernel(length, accepted, k_ref, v_ref, new_ref, ko_ref, vo_ref, kn, vn, kt, vt):
    b = pl.program_id(0)
    offset = (lax.axis_index("kv_0") * NY + lax.axis_index("kv_1")) * 32
    at = jnp.clip(length[b] + accepted[b] - offset + 16, 0, 48)
    for i in range(NY):
        for v in range(4):
            kn[pl.ds(i * 4 + v, 16, stride=16), :] = new_ref[0, i, 0, :, v * 128:(v + 1) * 128].astype(F32)
        for v in range(4):
            h, half = v // 2, v % 2
            vn[half, pl.ds(i * 2 + h, 16, stride=8), :] = new_ref[0, i, 0, :, 512 + v * 128:640 + v * 128].astype(F32)
    kt[16:48] = k_ref[0]
    vt[16:48] = v_ref[0]
    kt[pl.ds(at, 16)] = kn[...].reshape(16, 16, 128).astype(BF16)
    for half in range(2):
        vt[pl.ds(at, 16), :, half * 128:(half + 1) * 128] = vn[half].reshape(16, 8, 128).astype(BF16)
    ko_ref[0] = kt[16:48]
    vo_ref[0] = vt[16:48]


def insert(length, accepted, keys, values, new):
    def spec(*shape):
        return pl.BlockSpec((1, *shape), lambda b, *_: (b, 0, 0, 0))

    return pl.pallas_call(
        insert_kernel,
        name="insert",
        grid_spec=pltpu.PrefetchScalarGridSpec(
            num_scalar_prefetch=2,
            grid=(16,),
            in_specs=[
                spec(32, 16, 128), spec(32, 8, 256),
                pl.BlockSpec((1, NY, 1, 16, 1024), lambda b, *_: (b // 2, 0, b % 2, 0, 0)),
            ],
            out_specs=(spec(32, 16, 128), spec(32, 8, 256)),
            scratch_shapes=[
                pltpu.VMEM((256, 128), F32), pltpu.VMEM((2, 128, 128), F32),
                pltpu.VMEM((64, 16, 128), BF16), pltpu.VMEM((64, 8, 256), BF16),
            ],
        ),
        out_shape=(
            jax.ShapeDtypeStruct((16, 32, 16, 128), BF16),
            jax.ShapeDtypeStruct((16, 32, 8, 256), BF16),
        ),
    )(length, accepted, keys, values, new)


def per_device(tokens, in_gain, query_weight, key_weight, value_weight, out_weight, lambdas, sub_gain,
               key_cache, value_cache, cache_len, accepted, parents):
    frequency = np.float32(10000.0) ** (-np.arange(64, dtype=np.float32) / np.float32(64))
    frequency = jnp.asarray(np.concatenate([frequency, frequency])[None, :])
    output, new = layer(
        cache_len, accepted, lambdas, parents, tokens.reshape(256, 128), in_gain.reshape(1, 128),
        sub_gain.reshape(1, 256), frequency, query_weight, key_weight, value_weight,
        key_cache.reshape(16, 512, 128), value_cache.reshape(16, 256, 256), out_weight,
    )
    key_out, value_out = insert(
        cache_len, accepted, key_cache.reshape(16, 32, 16, 128), value_cache, new.reshape(NZ, NY, 2, 16, 1024)
    )
    return output.reshape(16, 16, 64), key_out.reshape(key_cache.shape), value_out


def solution(mesh):
    torus = Mesh(mesh.devices.reshape(mesh.shape["dp"], NZ, NY, mesh.shape["tp"]), ("dp", "kv_0", "kv_1", "tp"))
    placed = (
        P("dp", None, KV), P(KV), P(KV, "tp"), P(KV, "tp"), P(KV, "tp"), P("tp", KV), P("tp"), P(),
        P("dp", KV, "tp", None, None), P("dp", KV, "tp", None), P("dp"), P("dp"), P("dp", None),
    )
    return jax.shard_map(
        per_device, mesh=torus, in_specs=placed,
        out_specs=(P("dp", None, KV_TP), P("dp", KV, "tp", None, None), P("dp", KV, "tp", None)),
        check_vma=False,
    )
```

```python
import functools
import math

import jax
import jax.numpy as jnp
import numpy as np
from jax import lax
from jax.experimental import pallas as pl
from jax.experimental.pallas import tpu as pltpu
from jax.sharding import Mesh
from jax.sharding import PartitionSpec as P

D = 4096
NZ, NY = 8, 4
KV = ("kv_0", "kv_1")
KV_TP = ("kv_0", "kv_1", "tp")
LAMBDA_SCALE = 0.2 + 0.6 * math.exp(-0.6)
NEG_FILL = -1e30
ROOT = 128 ** (-0.5)
F32, BF16 = jnp.float32, jnp.bfloat16
MESH_ID = pl.DeviceIdType.MESH
DMA = pltpu.SemaphoreType.DMA
Z_STEPS = (1, 7, 2, 6, 3, 5, 4)
Y_STEPS = (1, 3, 2)


def places():
    return lax.axis_index("kv_0"), lax.axis_index("kv_1"), lax.axis_index("tp")


def remote(src, dst, send_sem, recv_sem, **where):
    return pltpu.make_async_remote_copy(
        src_ref=src, dst_ref=dst, send_sem=send_sem, recv_sem=recv_sem,
        device_id=where, device_id_type=MESH_ID,
    )


def greet(z, y, c, with_tp):
    barrier = pltpu.get_barrier_semaphore()
    for d in range(1, NZ):
        pl.semaphore_signal(barrier, inc=1, device_id={"kv_0": (z + d) % NZ}, device_id_type=MESH_ID)
    for d in range(1, NY):
        pl.semaphore_signal(barrier, inc=1, device_id={"kv_1": (y + d) % NY}, device_id_type=MESH_ID)
    if with_tp:
        pl.semaphore_signal(barrier, inc=1, device_id={"tp": 1 - c}, device_id_type=MESH_ID)
    pl.semaphore_wait(barrier, NZ - 1 + NY - 1 + int(with_tp))


def gather_2d(buf, z, y, zs, zr, ys, yr):
    def z_copy(d):
        return remote(buf.at[z, y], buf.at[z, y], zs.at[d], zr.at[d], kv_0=(z + d) % NZ)

    def y_copy(k, e):
        row = (z + NZ - k) % NZ
        return remote(buf.at[row, y], buf.at[row, y], ys.at[k, e - 1], yr.at[k, e - 1], kv_1=(y + e) % NY)

    def start():
        for d in Z_STEPS:
            z_copy(d).start()
        for e in Y_STEPS:
            y_copy(0, e).start()

    def hand_on(d):
        z_copy(d).wait_recv()
        for e in Y_STEPS:
            y_copy(d, e).start()

    def arrived(k):
        for e in Y_STEPS:
            y_copy(k, e).wait_recv()

    def end():
        for d in Z_STEPS:
            z_copy(d).wait_send()
        for k in (0, *Z_STEPS):
            for e in Y_STEPS:
                y_copy(k, e).wait_send()

    return start, hand_on, arrived, end


def contract(a, b, dims):
    return lax.dot_general(a, b, (dims, ((), ())), preferred_element_type=F32)


def layer_kernel(length, accepted, lambdas, parents, tok, gain, sub, freq, wq, wk, wv, keys_in, values_in, wo_in,
                 out, kg, vg,
                 tokg, gaing, wbuf, nrm, pq0, pq1, pkv, zq0, zq1, zkv, qg, kvown, knew, vnew, turn, kc, vc, wo, code, pscr, st, sx, mst, acc, accx,
                 yst, zst, gst, bs, ybuf, zsum, zbuf, mg, prod, got,
                 ls, ws, wr, ts, tr, gs, gr, qs, qr, ks, kr, azs, azr, ays, ayr, kzs, kzr, kys, kyr,
                 ss, sr, s2, r2, bss, bsr, zs, zr, xs, xr):
    z, y, c = places()
    loads = [
        pltpu.make_async_copy(src, dst, ls.at[3 + i])
        for i, (src, dst) in enumerate(((keys_in, kc), (values_in, vc), (wo_in, wo)))
    ]
    gaing[y] = jnp.broadcast_to(gain[...], (16, 128))
    greet(z, y, c, True)
    ws_in = (wq, wk, wv)

    def tok_copy(e):
        return remote(tok, tokg.at[y], ts.at[e], tr.at[e], kv_1=(y + e) % NY)

    def gain_copy(e):
        return remote(gaing.at[y], gaing.at[y], gs.at[e], gr.at[e], kv_1=(y + e) % NY)

    pieces = ((0, 0, 256), (0, 256, 256), (1, 0, 512), (2, 0, 512))

    def w_copy(i, e):
        to = (y + e) % NY
        m, first, size = pieces[i]
        cols = pl.ds(pl.multiple_of(to * 512 + first, 256), size)
        into = wbuf.at[m, y, :, first:first + size]
        return remote(ws_in[m].at[:, cols], into, ws.at[i, e], wr.at[i, e], kv_1=to)

    for e in Y_STEPS:
        gain_copy(e).start()
        tok_copy(e).start()
    for i in range(4):
        for e in Y_STEPS:
            w_copy(i, e).start()
    mine = pl.ds(pl.multiple_of(y * 512, 512), 512)
    own = [pltpu.make_async_copy(ws_in[m].at[:, mine], wbuf.at[m, y], ls.at[m]) for m in range(3)]
    for o in own:
        o.start()
    for load in loads:
        load.start()
    tokg[y] = tok[...]

    row16 = lax.broadcasted_iota(jnp.int32, (16, 16), 0)
    lane16 = lax.broadcasted_iota(jnp.int32, (16, 16), 1)
    unit = (row16 == lane16).astype(F32)
    spread16 = (lax.broadcasted_iota(jnp.int32, (16, 128), 1) % 16 == lax.broadcasted_iota(jnp.int32, (16, 128), 0)).astype(BF16)
    near = parents[pl.ds(2 * z, 2), :]
    seen, angles = [], []
    for s in range(2):
        reach = jnp.maximum(unit, (near[s:s + 1, :] == row16).astype(F32))
        for _ in range(4):
            half = reach.astype(BF16)
            reach = jnp.minimum(jnp.dot(half, half, preferred_element_type=F32), 1.0)
        half = reach.astype(BF16)
        seen.append(jnp.dot(half, spread16, preferred_element_type=F32))
        depth = contract(half, jnp.ones((16, 128), BF16), ((0,), (0,))) - 1.0
        begin = length[2 * z + s] + accepted[2 * z + s]
        angles.append((begin.astype(F32) + depth) * freq[...])
    angle = jnp.concatenate(angles, axis=0)
    cos = jnp.cos(angle)
    sin = jnp.where(lax.broadcasted_iota(jnp.int32, (32, 128), 1) < 64, -1.0, 1.0) * jnp.sin(angle)
    row = lax.broadcasted_iota(jnp.int32, (512, 128), 0)
    lane = lax.broadcasted_iota(jnp.int32, (512, 128), 1)
    code[...] = jnp.where(((row // 2) % 8) == (lane // 16), row // 16, 4096)

    for e in Y_STEPS:
        gain_copy(e).wait_recv()
        tok_copy(e).wait_recv()
    power = jnp.zeros((256, 1), F32)
    for a in range(NY):
        wide = tokg[a].astype(F32)
        power += jnp.sum(wide * wide, axis=-1, keepdims=True)
        nrm[:, a * 128:(a + 1) * 128] = (wide * gaing[a, 0:1].astype(F32)).astype(BF16)
    high = power.astype(BF16)
    rest = power - high.astype(F32)
    mid = rest.astype(BF16)
    low = (rest - mid.astype(F32)).astype(BF16)
    lane = lax.broadcasted_iota(jnp.int32, (256, 128), 1)
    terms = jnp.where(lane == 0, high.astype(F32), jnp.where(lane == 1, mid.astype(F32), low.astype(F32)))
    terms = jnp.where(lane < 3, terms, 0.0)
    pq0[:, :, 256:384] = terms.astype(BF16).reshape(NZ, 32, 128)

    def product(i):
        m, first, size = pieces[i]
        if first == 0:
            own[m].wait()
        for e in Y_STEPS:
            w_copy(i, e).wait_recv()
        total = jnp.zeros((256, size), F32)
        for a in range(NY):
            total += jnp.dot(
                nrm[:, a * 128:(a + 1) * 128], wbuf[m, a, :, first:first + size], preferred_element_type=F32
            )
        return total.astype(BF16).reshape(NZ, 32, size)

    halves = ((pq0, zq0), (pq1, zq1))

    def q_copy(i, d):
        to = (z + d) % NZ
        return remote(halves[i][0].at[to], halves[i][1].at[d], qs.at[i, d], qr.at[i, d], kv_0=to)

    def kv_copy(m, d):
        to = (z + d) % NZ
        return remote(pkv.at[m, to], zkv.at[m, d], ks.at[m, d], kr.at[m, d], kv_0=to)

    pq0[:, :, 0:256] = product(0)
    for d in Z_STEPS:
        q_copy(0, d).start()
    pq1[...] = product(1)
    for d in Z_STEPS:
        q_copy(1, d).start()
    pkv[0] = product(2)

    totals = []
    for i in range(2):
        total = halves[i][0][z].astype(F32)
        for d in Z_STEPS:
            q_copy(i, d).wait_recv()
            total += halves[i][1][d].astype(F32)
        totals.append(total)
    power = jnp.sum(totals[0][:, 256:384], axis=-1, keepdims=True)
    scale = lax.rsqrt(power / D + 1e-06)

    def turned(block):
        return block * cos + pltpu.roll(block, 64, 1) * sin

    for v in range(4):
        cols = slice(v * 128, (v + 1) * 128)
        block = turned(totals[v // 2][:, v % 2 * 128:v % 2 * 128 + 128] * scale).astype(BF16)
        qg[z, y, 0, :, cols] = block[0:16]
        qg[z, y, 1, :, cols] = block[16:32]
    q_start, q_hand_on, q_arrived, q_end = gather_2d(qg, z, y, azs, azr, ays, ayr)
    q_start()
    for d in Z_STEPS:
        kv_copy(0, d).start()
    for d in Z_STEPS:
        q_hand_on(d)
    pkv[1] = product(3)
    for d in Z_STEPS:
        kv_copy(1, d).start()

    def finished(m):
        total = pkv[m, z].astype(F32)
        for d in Z_STEPS:
            kv_copy(m, d).wait_recv()
            total += zkv[m, d].astype(F32)
        for v in range(4):
            block = total[:, v * 128:(v + 1) * 128] * scale
            if m == 0:
                block = turned(block)
            at = m * 512 + v * 128
            kvown[:, at:at + 128] = block.astype(BF16)
            turn[m, pl.ds((v % 2) * 2 + v // 2 if m else v, 32, stride=4), :] = block

    upper = z >= NZ // 2

    pairs = ((knew, kg), (vnew, vg))

    def up_z(m, d):
        return remote(pairs[m][0], pairs[m][1].at[z, y], kzs.at[m, d], kzr.at[m, d], kv_0=(z + d) % NZ)

    def up_y(m, k, e):
        block = pairs[m][1].at[(z + NZ - k) % NZ, y]
        return remote(block, block, kys.at[m, k, e - 1], kyr.at[m, k, e - 1], kv_1=(y + e) % NY)

    own_up = [pltpu.make_async_copy(pairs[m][0], pairs[m][1].at[z, y], ls.at[6 + m]) for m in range(2)]

    def relay(m, k):
        at, to = (z + NZ - k) % NZ, (y + (1, 3)[m]) % NY
        block = pairs[m][1].at[at, (y + (3, 1)[m]) % NY]
        return remote(block, block, kys.at[m, k, 1], kyr.at[m, k, 1], kv_1=to)

    def to_upper(m, act):
        for d in Z_STEPS:
            @pl.when((z + d) % NZ >= NZ // 2)
            def _():
                act(up_z(m, d))

    def go_up(m):
        to_upper(m, lambda copy: copy.start())

        @pl.when(upper)
        def _():
            own_up[m].start()

    def hand_up(m):
        @pl.when(upper)
        def _():
            own_up[m].wait()
            for k in (0, *Z_STEPS):
                if k:
                    up_z(m, k).wait_recv()
                for e in (1, 3):
                    up_y(m, k, e).start()

    def hand_over(m):
        @pl.when(upper)
        def _():
            for k in (0, *Z_STEPS):
                up_y(m, k, (1, 3)[m]).wait_recv()
                relay(m, k).start()

    loads[0].wait()
    loads[1].wait()

    def queries_of(zc, s):
        return jnp.concatenate(
            [qg[zc, i, s, :, (h * 2 + m) * 128:(h * 2 + m + 1) * 128] for m in range(2) for i in range(NY) for h in range(2)],
            axis=0,
        )

    odd = lax.broadcasted_iota(jnp.int32, (8, 128), 0) % 2 == 1
    offset = (z * NY + y) * 32

    def nth(step):
        return jnp.where(step % 2 == 1, (step + 1) // 2, (NZ - step // 2) % NZ)

    def attend(step, carry):
        k = nth(step)
        q_arrived(k)
        zc = (z + NZ - k) % NZ
        for s in range(2):
            b = 2 * zc + s
            limit = length[b] + accepted[b] - offset
            both = contract(kc[b], queries_of(zc, s), ((1,), (1,)))
            both = both.reshape(64, 8, 256)
            live = (code[...] < limit).reshape(64, 8, 128)
            score = jnp.where(odd[None], both[:, :, 128:], both[:, :, :128]) * ROOT
            score = jnp.where(live, score, NEG_FILL)
            top = jnp.max(score, axis=0)
            peaks = [jnp.max(jnp.where(odd == bool(m), top, NEG_FILL), axis=0, keepdims=True) for m in range(2)]
            peak = jnp.where(odd, peaks[1], peaks[0])
            grown = jnp.where(live, jnp.exp(score - peak[None]), 0.0)
            part = jnp.sum(grown, axis=0)
            for m in range(2):
                st[0, zc, 2 * s + m:2 * s + m + 1] = peaks[m]
                st[1, zc, 2 * s + m:2 * s + m + 1] = jnp.sum(jnp.where(odd == bool(m), part, 0.0), axis=0, keepdims=True)
            pscr[s] = grown.reshape(512, 128)
            chance = jnp.concatenate([pscr[s, pl.ds(m, 256, stride=2), :] for m in range(2)], axis=1).astype(BF16)
            acc[zc, s] = contract(chance, vc[b], ((0,), (0,))).astype(BF16)
        return carry

    lax.fori_loop(0, NZ - 2, attend, 0)
    finished(0)
    knew[...] = turn[0].astype(BF16).reshape(32, 4, 128)
    go_up(0)

    lax.fori_loop(NZ - 2, NZ, attend, 0)
    q_end()
    finished(1)
    vnew[...] = turn[1].astype(BF16).reshape(32, 2, 2, 128)
    go_up(1)

    head_row = 2 * y + lax.broadcasted_iota(jnp.int32, (32, 128), 0) // 16
    head_lane = lax.broadcasted_iota(jnp.int32, (32, 128), 1) // 16
    for s in range(2):
        rows = slice(s * 16, (s + 1) * 16)
        keys = jnp.concatenate(
            [kvown[rows, (h * 2 + m) * 128:(h * 2 + m + 1) * 128] for m in range(2) for h in range(2)], axis=0
        )
        values = jnp.concatenate([kvown[rows, 512:768], kvown[rows, 768:1024]], axis=0)
        both = contract(keys, queries_of(z, s), ((1,), (1,)))
        live = (head_row == head_lane) & (jnp.concatenate([seen[s], seen[s]], axis=0) > 0.5)
        chance = []
        for m in range(2):
            score = jnp.where(live, both[m * 32:(m + 1) * 32, m * 128:(m + 1) * 128] * ROOT, NEG_FILL)
            peak = jnp.max(score, axis=0, keepdims=True)
            grown = jnp.where(live, jnp.exp(score - peak), 0.0)
            sx[0, 2 * s + m:2 * s + m + 1] = peak
            sx[1, 2 * s + m:2 * s + m + 1] = jnp.sum(grown, axis=0, keepdims=True)
            chance.append(grown)
        accx[s] = contract(jnp.concatenate(chance, axis=1).astype(BF16), values, ((0,), (0,))).astype(BF16)
    def log_sum(peak, total):
        return peak + jnp.log(jnp.maximum(total, 1e-30))

    def joined(parts):
        peak = functools.reduce(jnp.maximum, parts)
        return log_sum(peak, sum(jnp.exp(part - peak) for part in parts))

    mst[...] = log_sum(st[0], st[1])
    mst[z] = joined([mst[z], log_sum(sx[0], sx[1])])

    def st_copy(e):
        return remote(mst, yst.at[e], ss.at[e], sr.at[e], kv_1=(y + e) % NY)

    for e in Y_STEPS:
        st_copy(e).start()
    parts = [mst[...]]
    for e in Y_STEPS:
        st_copy(e).wait_recv()
        parts.append(yst[e])
    zst[0] = joined(parts)

    def st_z(d):
        return remote(zst.at[0], zst.at[d], s2.at[d], r2.at[d], kv_0=(z + d) % NZ)

    for d in Z_STEPS:
        st_z(d).start()
    hand_up(0)
    row = lax.broadcasted_iota(jnp.int32, (128, 128), 0)
    lane = lax.broadcasted_iota(jnp.int32, (128, 128), 1)
    same = row == lane
    lane = lax.broadcasted_iota(jnp.int32, (1, 128), 1) // 16
    lam = jnp.zeros((1, 128), F32)
    for h in range(8):
        lam = jnp.where(lane == h, -lambdas[h], lam)
    for d in Z_STEPS:
        st_z(d).wait_recv()
    gst[...] = joined([zst[d] for d in range(NZ)])

    def b_copy(zc, e):
        to = (y + e) % NY
        return remote(bs.at[to, zc], ybuf.at[e - 1, zc], bss.at[zc, e - 1], bsr.at[zc, e - 1], kv_1=to)

    def send_z(d):
        to = (z + d) % NZ
        return remote(zsum.at[to], zbuf.at[d], zs.at[d], zr.at[d], kv_0=to)

    def mixing(peaks, zc, s):
        ratio = jnp.exp(peaks - gst[zc])
        first = jnp.where(same, ratio[2 * s:2 * s + 1], 0.0)
        second = jnp.where(same, ratio[2 * s + 1:2 * s + 2] * lam, 0.0)
        return jnp.concatenate([first, second], axis=1).astype(BF16)

    def send_blocks(zc, last):
        for s in range(2):
            block = jnp.dot(mixing(st[0, zc], zc, s), acc[zc, s], preferred_element_type=F32)
            if last:
                block += jnp.dot(mixing(sx[0], zc, s), accx[s], preferred_element_type=F32)
            block = block.astype(BF16)
            for i in range(NY):
                bs[i, zc, s] = block[i * 32:(i + 1) * 32]
        for e in Y_STEPS:
            b_copy(zc, e).start()

    def blocks(d, carry):
        send_blocks((z + d) % NZ, False)
        return carry

    lax.fori_loop(1, NZ, blocks, 0)
    send_blocks(z, True)
    def sums(d, carry):
        zc = (z + d) % NZ
        total = bs[y, zc].astype(F32)
        for e in Y_STEPS:
            b_copy(zc, e).wait_recv()
            total += ybuf[e - 1, zc].astype(F32)
        zsum[zc] = total.astype(BF16)

        @pl.when(d < NZ)
        def _():
            send_z(d).start()

        return carry

    lax.fori_loop(1, NZ + 1, sums, 0)
    hand_up(1)
    hand_over(0)
    total = zsum[z].astype(F32)
    for d in range(1, NZ):
        send_z(d).wait_recv()
        total += zbuf[d].astype(F32)
    norm = total * lax.rsqrt(jnp.mean(total * total, axis=-1, keepdims=True) + 1e-05)
    mg[z, y] = (norm * sub[...].astype(F32).reshape(1, 256) * LAMBDA_SCALE).astype(BF16)
    m_start, m_hand_on, m_arrived, m_end = gather_2d(mg, z, y, azs, azr, ays, ayr)
    m_start()
    for d in Z_STEPS:
        m_hand_on(d)
    hand_over(1)
    loads[2].wait()
    for k in (0, *Z_STEPS):
        m_arrived(k)
    result = jnp.zeros((256, 128), F32)
    for h in range(8):
        i, k = h // 2, h % 2
        rows = jnp.concatenate(
            [mg[a, i, s, k * 16:(k + 1) * 16] for a in range(NZ) for s in range(2)], axis=0
        )
        result += jnp.dot(rows, wo[h * 256:(h + 1) * 256], preferred_element_type=F32)
    prod[...] = result.astype(BF16)
    swap = remote(prod, got, xs, xr, tp=1 - c)
    swap.start()
    swap.wait()
    result = prod[...].astype(F32) + got[...].astype(F32)
    out[...] = jnp.where(c == 0, result[:, 0:64], result[:, 64:128]).astype(BF16)

    for e in Y_STEPS:
        gain_copy(e).wait_send()
        tok_copy(e).wait_send()
        st_copy(e).wait_send()
        for i in range(4):
            w_copy(i, e).wait_send()
    for d in Z_STEPS:
        for i in range(2):
            q_copy(i, d).wait_send()
        for m in range(2):
            kv_copy(m, d).wait_send()
        st_z(d).wait_send()
        send_z(d).wait_send()

    m_end()
    for m in range(2):
        to_upper(m, lambda copy: copy.wait_send())

    def drain(zc, carry):
        for e in Y_STEPS:
            b_copy(zc, e).wait_send()
        return carry

    lax.fori_loop(0, NZ, drain, 0)

    @pl.when(upper)
    def _():
        for m in range(2):
            for k in (0, *Z_STEPS):
                up_y(m, k, 1).wait_send()
                up_y(m, k, 3).wait_send()
                up_y(m, k, (3, 1)[m]).wait_recv()
                relay(m, k).wait()


def layer(*operands):
    vmem, smem = pl.BlockSpec(memory_space=pltpu.VMEM), pl.BlockSpec(memory_space=pltpu.SMEM)
    anywhere = pl.BlockSpec(memory_space=pltpu.HBM)
    y_pair, z_pair = [DMA((NY,))] * 2, [DMA((NZ,))] * 2
    zy_pair = [DMA((NZ, NY - 1))] * 2
    return pl.pallas_call(
        layer_kernel,
        name="layer",
        out_shape=(
            jax.ShapeDtypeStruct((256, 64), BF16),
            jax.ShapeDtypeStruct((NZ, NY, 32, 4, 128), BF16),
            jax.ShapeDtypeStruct((NZ, NY, 32, 2, 2, 128), BF16),
        ),
        in_specs=[smem] * 3 + [vmem] * 8 + [anywhere] * 3,
        out_specs=(vmem, anywhere, anywhere),
        scratch_shapes=[
            pltpu.VMEM((NY, 256, 128), BF16),
            pltpu.VMEM((NY, 16, 128), BF16),
            pltpu.VMEM((3, NY, 128, 512), BF16),
            pltpu.VMEM((256, 512), BF16),
            pltpu.VMEM((NZ, 32, 384), BF16),
            pltpu.VMEM((NZ, 32, 256), BF16),
            pltpu.VMEM((2, NZ, 32, 512), BF16),
            pltpu.VMEM((NZ, 32, 384), BF16),
            pltpu.VMEM((NZ, 32, 256), BF16),
            pltpu.VMEM((2, NZ, 32, 512), BF16),
            pltpu.VMEM((NZ, NY, 2, 16, 512), BF16),
            pltpu.VMEM((32, 1024), BF16),
            pltpu.VMEM((32, 4, 128), BF16),
            pltpu.VMEM((32, 2, 2, 128), BF16),
            pltpu.VMEM((2, 128, 128), F32),
            pltpu.VMEM((16, 512, 128), BF16),
            pltpu.VMEM((16, 256, 256), BF16),
            pltpu.VMEM((2048, 128), BF16),
            pltpu.VMEM((512, 128), jnp.int32),
            pltpu.VMEM((2, 512, 128), F32),
            pltpu.VMEM((2, NZ, 4, 128), F32),
            pltpu.VMEM((2, 4, 128), F32),
            pltpu.VMEM((NZ, 4, 128), F32),
            pltpu.VMEM((NZ, 2, 256, 256), BF16),
            pltpu.VMEM((2, 256, 256), BF16),
            pltpu.VMEM((NY, NZ, 4, 128), F32),
            pltpu.VMEM((NZ, NZ, 4, 128), F32),
            pltpu.VMEM((NZ, 4, 128), F32),
            pltpu.VMEM((NY, NZ, 2, 32, 256), BF16),
            pltpu.VMEM((NY - 1, NZ, 2, 32, 256), BF16),
            pltpu.VMEM((NZ, 2, 32, 256), BF16),
            pltpu.VMEM((NZ, 2, 32, 256), BF16),
            pltpu.VMEM((NZ, NY, 2, 32, 256), BF16),
            pltpu.VMEM((256, 128), BF16),
            pltpu.VMEM((256, 128), BF16),
            DMA((8,)), DMA((4, NY)), DMA((4, NY)), *y_pair, *y_pair,
            DMA((2, NZ)), DMA((2, NZ)), DMA((2, NZ)), DMA((2, NZ)),
            *z_pair, *zy_pair, DMA((2, NZ)), DMA((2, NZ)), DMA((2, NZ, NY - 1)), DMA((2, NZ, NY - 1)),
            *y_pair, *z_pair, *zy_pair, *z_pair, DMA, DMA,
        ],
        compiler_params=pltpu.CompilerParams(
            collective_id=0, has_side_effects=True, vmem_limit_bytes=56 * 1024 * 1024
        ),
    )(*operands)


def insert_kernel(length, accepted, k_in, v_in, kg, vg, ko, vo, kt, vt, ins, new, outs):
    z, y, _ = places()
    offset = (z * NY + y) * 32

    def load(b):
        return (
            pltpu.make_async_copy(k_in.at[b], kt.at[b, 16:48], ins.at[0, b]),
            pltpu.make_async_copy(v_in.at[b], vt.at[b, 16:48], ins.at[1, b]),
        )

    def place(b):
        at = pl.ds(jnp.clip(length[b] + accepted[b] - offset + 16, 0, 48), 16)
        rows = pl.ds((b % 2) * 16, 16)
        return [
            pltpu.make_async_copy(kg.at[b // 2, i, rows], kt.at[b, at, i], new.at[0, b, i]) for i in range(NY)
        ] + [
            pltpu.make_async_copy(vg.at[b // 2, i, rows], vt.at[b, at, :, i], new.at[1, b, i]) for i in range(NY)
        ]

    def store(b):
        return (
            pltpu.make_async_copy(kt.at[b, 16:48], ko.at[b], outs.at[0, b]),
            pltpu.make_async_copy(vt.at[b, 16:48], vo.at[b], outs.at[1, b]),
        )

    def each(body):
        def step(b, carry):
            body(b)
            return carry

        lax.fori_loop(0, 16, step, 0)

    def act(copies, name):
        for copy in copies:
            getattr(copy, name)()

    each(lambda b: act(load(b), "start"))

    @pl.when(z >= NZ // 2)
    def _():
        def body(b):
            act(load(b), "wait")
            act(place(b), "start")

        each(body)

        def body(b):
            act(place(b), "wait")
            act(store(b), "start")

        each(body)

    @pl.when(z < NZ // 2)
    def _():
        def body(b):
            act(load(b), "wait")
            act(store(b), "start")

        each(body)

    each(lambda b: act(store(b), "wait"))


def insert(length, accepted, keys, values, new_keys, new_values):
    smem, anywhere = pl.BlockSpec(memory_space=pltpu.SMEM), pl.BlockSpec(memory_space=pltpu.HBM)
    return pl.pallas_call(
        insert_kernel,
        name="insert",
        in_specs=[smem] * 2 + [anywhere] * 4,
        out_specs=(anywhere, anywhere),
        scratch_shapes=[
            pltpu.VMEM((16, 64, NY, 4, 128), BF16), pltpu.VMEM((16, 64, 2, NY, 2, 128), BF16),
            DMA((2, 16)), DMA((2, 16, NY)), DMA((2, 16)),
        ],
        out_shape=(
            jax.ShapeDtypeStruct((16, 32, NY, 4, 128), BF16),
            jax.ShapeDtypeStruct((16, 32, 2, NY, 2, 128), BF16),
        ),
        compiler_params=pltpu.CompilerParams(vmem_limit_bytes=62 * 1024 * 1024),
    )(length, accepted, keys, values, new_keys, new_values)


def per_device(tokens, in_gain, query_weight, key_weight, value_weight, out_weight, lambdas, sub_gain,
               key_cache, value_cache, cache_len, accepted, parents):
    frequency = np.float32(10000.0) ** (-np.arange(64, dtype=np.float32) / np.float32(64))
    frequency = jnp.asarray(np.concatenate([frequency, frequency])[None, :])
    output, new_keys, new_values = layer(
        cache_len, accepted, lambdas, parents, tokens.reshape(256, 128), in_gain.reshape(1, 128),
        sub_gain, frequency, query_weight, key_weight, value_weight,
        key_cache.reshape(16, 512, 128), value_cache.reshape(16, 256, 256), out_weight,
    )
    values = value_cache.reshape(16, 32, NY, 2, 2, 128).transpose(0, 1, 4, 2, 3, 5)
    key_out, value_out = insert(
        cache_len, accepted, key_cache.reshape(16, 32, NY, 4, 128), values, new_keys, new_values
    )
    value_out = value_out.transpose(0, 1, 3, 4, 2, 5).reshape(value_cache.shape)
    return output.reshape(16, 16, 64), key_out.reshape(key_cache.shape), value_out


def solution(mesh):
    torus = Mesh(mesh.devices.reshape(mesh.shape["dp"], NZ, NY, mesh.shape["tp"]), ("dp", "kv_0", "kv_1", "tp"))
    placed = (
        P("dp", None, KV), P(KV), P(KV, "tp"), P(KV, "tp"), P(KV, "tp"), P("tp", KV), P("tp"), P(),
        P("dp", KV, "tp", None, None), P("dp", KV, "tp", None), P("dp"), P("dp"), P("dp", None),
    )
    return jax.shard_map(
        per_device, mesh=torus, in_specs=placed,
        out_specs=(P("dp", None, KV_TP), P("dp", KV, "tp", None, None), P("dp", KV, "tp", None)),
        check_vma=False,
    )
```

```python
import functools
import math

import jax
import jax.numpy as jnp
import numpy as np
from jax import lax
from jax.experimental import pallas as pl
from jax.experimental.pallas import tpu as pltpu
from jax.sharding import Mesh
from jax.sharding import PartitionSpec as P

D = 4096
NZ, NY = 8, 4
KV = ("kv_0", "kv_1")
KV_TP = ("kv_0", "kv_1", "tp")
LAMBDA_SCALE = 0.2 + 0.6 * math.exp(-0.6)
NEG_FILL = -1e30
ROOT = 128 ** (-0.5)
F32, BF16 = jnp.float32, jnp.bfloat16
MESH_ID = pl.DeviceIdType.MESH
DMA = pltpu.SemaphoreType.DMA
Z_STEPS = (1, 7, 2, 6, 3, 5, 4)
Y_STEPS = (1, 3, 2)
FAR_FIRST = (4, 3, 5, 2, 6, 1, 7)


def places():
    return lax.axis_index("kv_0"), lax.axis_index("kv_1"), lax.axis_index("tp")


def remote(src, dst, send_sem, recv_sem, **where):
    return pltpu.make_async_remote_copy(
        src_ref=src, dst_ref=dst, send_sem=send_sem, recv_sem=recv_sem,
        device_id=where, device_id_type=MESH_ID,
    )


def greet(z, y, c, with_tp):
    barrier = pltpu.get_barrier_semaphore()
    for d in range(1, NZ):
        pl.semaphore_signal(barrier, inc=1, device_id={"kv_0": (z + d) % NZ}, device_id_type=MESH_ID)
    for d in range(1, NY):
        pl.semaphore_signal(barrier, inc=1, device_id={"kv_1": (y + d) % NY}, device_id_type=MESH_ID)
    if with_tp:
        pl.semaphore_signal(barrier, inc=1, device_id={"tp": 1 - c}, device_id_type=MESH_ID)
    pl.semaphore_wait(barrier, NZ - 1 + NY - 1 + int(with_tp))


def gather_2d(buf, z, y, zs, zr, ys, yr):
    def z_copy(d):
        return remote(buf.at[z, y], buf.at[z, y], zs.at[d], zr.at[d], kv_0=(z + d) % NZ)

    def y_copy(k, e):
        row = (z + NZ - k) % NZ
        return remote(buf.at[row, y], buf.at[row, y], ys.at[k, e - 1], yr.at[k, e - 1], kv_1=(y + e) % NY)

    def start():
        for d in Z_STEPS:
            z_copy(d).start()
        for e in Y_STEPS:
            y_copy(0, e).start()

    def hand_on(d):
        z_copy(d).wait_recv()
        for e in Y_STEPS:
            y_copy(d, e).start()

    def arrived(k):
        for e in Y_STEPS:
            y_copy(k, e).wait_recv()

    def end():
        for d in Z_STEPS:
            z_copy(d).wait_send()
        for k in (0, *Z_STEPS):
            for e in Y_STEPS:
                y_copy(k, e).wait_send()

    return start, hand_on, arrived, end


def contract(a, b, dims):
    return lax.dot_general(a, b, (dims, ((), ())), preferred_element_type=F32)


def layer_kernel(length, accepted, lambdas, parents, tok, gain, sub, freq, wq, wk, wv, keys_in, values_in, wo_in,
                 out, kg, vg,
                 tokg, gaing, wbuf, nrm, pq0, pq1, pkv, zq0, zq1, zkv, qg, kvown, knew, vnew, turn, kc, vc, wo, code, pscr, st, sx, mst, acc, accx,
                 yst, zst, gst, bs, ybuf, zsum, zbuf, mg, prod, got,
                 ls, ws, wr, ts, tr, gs, gr, qs, qr, ks, kr, azs, azr, ays, ayr, kzs, kzr, kys, kyr,
                 ss, sr, s2, r2, bss, bsr, zs, zr, xs, xr):
    z, y, c = places()
    loads = [
        pltpu.make_async_copy(src, dst, ls.at[3 + i])
        for i, (src, dst) in enumerate(((keys_in, kc), (values_in, vc), (wo_in, wo)))
    ]
    gaing[y] = jnp.broadcast_to(gain[...], (16, 128))
    greet(z, y, c, True)
    ws_in = (wq, wk, wv)

    def tok_copy(e):
        return remote(tok, tokg.at[y], ts.at[e], tr.at[e], kv_1=(y + e) % NY)

    def gain_copy(e):
        return remote(gaing.at[y], gaing.at[y], gs.at[e], gr.at[e], kv_1=(y + e) % NY)

    pieces = ((0, 0, 256), (0, 256, 256), (1, 0, 512), (2, 0, 512))

    def w_copy(i, e):
        to = (y + e) % NY
        m, first, size = pieces[i]
        cols = pl.ds(pl.multiple_of(to * 512 + first, 256), size)
        into = wbuf.at[m, y, :, first:first + size]
        return remote(ws_in[m].at[:, cols], into, ws.at[i, e], wr.at[i, e], kv_1=to)

    for e in Y_STEPS:
        gain_copy(e).start()
        tok_copy(e).start()
    for i in range(4):
        for e in Y_STEPS:
            w_copy(i, e).start()
    mine = pl.ds(pl.multiple_of(y * 512, 512), 512)
    own = [pltpu.make_async_copy(ws_in[m].at[:, mine], wbuf.at[m, y], ls.at[m]) for m in range(3)]
    for o in own:
        o.start()
    for load in loads:
        load.start()
    tokg[y] = tok[...]

    row16 = lax.broadcasted_iota(jnp.int32, (16, 16), 0)
    lane16 = lax.broadcasted_iota(jnp.int32, (16, 16), 1)
    unit = (row16 == lane16).astype(F32)
    spread16 = (lax.broadcasted_iota(jnp.int32, (16, 128), 1) % 16 == lax.broadcasted_iota(jnp.int32, (16, 128), 0)).astype(BF16)
    near = parents[pl.ds(2 * z, 2), :]
    seen, angles = [], []
    for s in range(2):
        reach = jnp.maximum(unit, (near[s:s + 1, :] == row16).astype(F32))
        for _ in range(4):
            half = reach.astype(BF16)
            reach = jnp.minimum(jnp.dot(half, half, preferred_element_type=F32), 1.0)
        half = reach.astype(BF16)
        seen.append(jnp.dot(half, spread16, preferred_element_type=F32))
        depth = contract(half, jnp.ones((16, 128), BF16), ((0,), (0,))) - 1.0
        begin = length[2 * z + s] + accepted[2 * z + s]
        angles.append((begin.astype(F32) + depth) * freq[...])
    angle = jnp.concatenate(angles, axis=0)
    cos = jnp.cos(angle)
    sin = jnp.where(lax.broadcasted_iota(jnp.int32, (32, 128), 1) < 64, -1.0, 1.0) * jnp.sin(angle)
    row = lax.broadcasted_iota(jnp.int32, (512, 128), 0)
    lane = lax.broadcasted_iota(jnp.int32, (512, 128), 1)
    code[...] = jnp.where(((row // 2) % 8) == (lane // 16), row // 16, 4096)

    for e in Y_STEPS:
        gain_copy(e).wait_recv()
        tok_copy(e).wait_recv()
    power = jnp.zeros((256, 1), F32)
    for a in range(NY):
        wide = tokg[a].astype(F32)
        power += jnp.sum(wide * wide, axis=-1, keepdims=True)
        nrm[:, a * 128:(a + 1) * 128] = (wide * gaing[a, 0:1].astype(F32)).astype(BF16)
    high = power.astype(BF16)
    rest = power - high.astype(F32)
    mid = rest.astype(BF16)
    low = (rest - mid.astype(F32)).astype(BF16)
    lane = lax.broadcasted_iota(jnp.int32, (256, 128), 1)
    terms = jnp.where(lane == 0, high.astype(F32), jnp.where(lane == 1, mid.astype(F32), low.astype(F32)))
    terms = jnp.where(lane < 3, terms, 0.0)
    pq0[:, :, 256:384] = terms.astype(BF16).reshape(NZ, 32, 128)

    def product(i):
        m, first, size = pieces[i]
        if first == 0:
            own[m].wait()
        for e in Y_STEPS:
            w_copy(i, e).wait_recv()
        total = jnp.zeros((256, size), F32)
        for a in range(NY):
            total += jnp.dot(
                nrm[:, a * 128:(a + 1) * 128], wbuf[m, a, :, first:first + size], preferred_element_type=F32
            )
        return total.astype(BF16).reshape(NZ, 32, size)

    halves = ((pq0, zq0), (pq1, zq1))

    def q_copy(i, d):
        to = (z + d) % NZ
        return remote(halves[i][0].at[to], halves[i][1].at[d], qs.at[i, d], qr.at[i, d], kv_0=to)

    def kv_copy(m, d):
        to = (z + d) % NZ
        return remote(pkv.at[m, to], zkv.at[m, d], ks.at[m, d], kr.at[m, d], kv_0=to)

    pq0[:, :, 0:256] = product(0)
    for d in FAR_FIRST:
        q_copy(0, d).start()
    pq1[...] = product(1)
    for d in FAR_FIRST:
        q_copy(1, d).start()
    pkv[0] = product(2)
    for d in FAR_FIRST:
        kv_copy(0, d).start()

    totals = []
    for i in range(2):
        total = halves[i][0][z].astype(F32)
        for d in Z_STEPS:
            q_copy(i, d).wait_recv()
            total += halves[i][1][d].astype(F32)
        totals.append(total)
    power = jnp.sum(totals[0][:, 256:384], axis=-1, keepdims=True)
    scale = lax.rsqrt(power / D + 1e-06)

    def turned(block):
        return block * cos + pltpu.roll(block, 64, 1) * sin

    for v in range(4):
        cols = slice(v * 128, (v + 1) * 128)
        block = turned(totals[v // 2][:, v % 2 * 128:v % 2 * 128 + 128] * scale).astype(BF16)
        qg[z, y, 0, :, cols] = block[0:16]
        qg[z, y, 1, :, cols] = block[16:32]
    q_start, q_hand_on, q_arrived, q_end = gather_2d(qg, z, y, azs, azr, ays, ayr)
    q_start()
    for d in Z_STEPS:
        q_hand_on(d)
    def finished(m):
        total = pkv[m, z].astype(F32)
        for d in Z_STEPS:
            kv_copy(m, d).wait_recv()
            total += zkv[m, d].astype(F32)
        for v in range(4):
            block = total[:, v * 128:(v + 1) * 128] * scale
            if m == 0:
                block = turned(block)
            at = m * 512 + v * 128
            kvown[:, at:at + 128] = block.astype(BF16)
            turn[m, pl.ds((v % 2) * 2 + v // 2 if m else v, 32, stride=4), :] = block

    upper = z >= NZ // 2

    pairs = ((knew, kg), (vnew, vg))

    def up_z(m, d):
        return remote(pairs[m][0], pairs[m][1].at[z, y], kzs.at[m, d], kzr.at[m, d], kv_0=(z + d) % NZ)

    def up_y(m, k, e):
        block = pairs[m][1].at[(z + NZ - k) % NZ, y]
        return remote(block, block, kys.at[m, k, e - 1], kyr.at[m, k, e - 1], kv_1=(y + e) % NY)

    own_up = [pltpu.make_async_copy(pairs[m][0], pairs[m][1].at[z, y], ls.at[6 + m]) for m in range(2)]

    def relay(m, k):
        at, to = (z + NZ - k) % NZ, (y + (1, 3)[m]) % NY
        block = pairs[m][1].at[at, (y + (3, 1)[m]) % NY]
        return remote(block, block, kys.at[m, k, 1], kyr.at[m, k, 1], kv_1=to)

    def to_upper(m, act):
        for d in Z_STEPS:
            @pl.when((z + d) % NZ >= NZ // 2)
            def _():
                act(up_z(m, d))

    def go_up(m):
        to_upper(m, lambda copy: copy.start())

        @pl.when(upper)
        def _():
            own_up[m].start()

    def hand_up(m):
        @pl.when(upper)
        def _():
            own_up[m].wait()
            for k in (0, *Z_STEPS):
                if k:
                    up_z(m, k).wait_recv()
                for e in (1, 3):
                    up_y(m, k, e).start()

    def hand_over(m):
        @pl.when(upper)
        def _():
            for k in (0, *Z_STEPS):
                up_y(m, k, (1, 3)[m]).wait_recv()
                relay(m, k).start()

    finished(0)
    knew[...] = turn[0].astype(BF16).reshape(32, 4, 128)
    go_up(0)
    pkv[1] = product(3)
    for d in Z_STEPS:
        kv_copy(1, d).start()

    loads[0].wait()
    loads[1].wait()

    def queries_of(zc, s):
        return jnp.concatenate(
            [qg[zc, i, s, :, (h * 2 + m) * 128:(h * 2 + m + 1) * 128] for m in range(2) for i in range(NY) for h in range(2)],
            axis=0,
        )

    odd = lax.broadcasted_iota(jnp.int32, (8, 128), 0) % 2 == 1
    offset = (z * NY + y) * 32

    def nth(step):
        return jnp.where(step % 2 == 1, (step + 1) // 2, (NZ - step // 2) % NZ)

    def attend(step, carry):
        k = nth(step)
        q_arrived(k)
        zc = (z + NZ - k) % NZ
        for s in range(2):
            b = 2 * zc + s
            limit = length[b] + accepted[b] - offset
            both = contract(kc[b], queries_of(zc, s), ((1,), (1,)))
            both = both.reshape(64, 8, 256)
            live = (code[...] < limit).reshape(64, 8, 128)
            score = jnp.where(odd[None], both[:, :, 128:], both[:, :, :128]) * ROOT
            score = jnp.where(live, score, NEG_FILL)
            top = jnp.max(score, axis=0)
            peaks = [jnp.max(jnp.where(odd == bool(m), top, NEG_FILL), axis=0, keepdims=True) for m in range(2)]
            peak = jnp.where(odd, peaks[1], peaks[0])
            grown = jnp.where(live, jnp.exp(score - peak[None]), 0.0)
            part = jnp.sum(grown, axis=0)
            for m in range(2):
                st[0, zc, 2 * s + m:2 * s + m + 1] = peaks[m]
                st[1, zc, 2 * s + m:2 * s + m + 1] = jnp.sum(jnp.where(odd == bool(m), part, 0.0), axis=0, keepdims=True)
            pscr[s] = grown.reshape(512, 128)
            chance = jnp.concatenate([pscr[s, pl.ds(m, 256, stride=2), :] for m in range(2)], axis=1).astype(BF16)
            acc[zc, s] = contract(chance, vc[b], ((0,), (0,))).astype(BF16)
        return carry

    lax.fori_loop(0, NZ, attend, 0)
    q_end()

    weights = []
    head_row = 2 * y + lax.broadcasted_iota(jnp.int32, (32, 128), 0) // 16
    head_lane = lax.broadcasted_iota(jnp.int32, (32, 128), 1) // 16
    for s in range(2):
        rows = slice(s * 16, (s + 1) * 16)
        keys = jnp.concatenate(
            [kvown[rows, (h * 2 + m) * 128:(h * 2 + m + 1) * 128] for m in range(2) for h in range(2)], axis=0
        )
        both = contract(keys, queries_of(z, s), ((1,), (1,)))
        live = (head_row == head_lane) & (jnp.concatenate([seen[s], seen[s]], axis=0) > 0.5)
        chance = []
        for m in range(2):
            score = jnp.where(live, both[m * 32:(m + 1) * 32, m * 128:(m + 1) * 128] * ROOT, NEG_FILL)
            peak = jnp.max(score, axis=0, keepdims=True)
            grown = jnp.where(live, jnp.exp(score - peak), 0.0)
            sx[0, 2 * s + m:2 * s + m + 1] = peak
            sx[1, 2 * s + m:2 * s + m + 1] = jnp.sum(grown, axis=0, keepdims=True)
            chance.append(grown)
        weights.append(jnp.concatenate(chance, axis=1).astype(BF16))
    def log_sum(peak, total):
        return peak + jnp.log(jnp.maximum(total, 1e-30))

    def joined(parts):
        peak = functools.reduce(jnp.maximum, parts)
        return log_sum(peak, sum(jnp.exp(part - peak) for part in parts))

    mst[...] = log_sum(st[0], st[1])
    mst[z] = joined([mst[z], log_sum(sx[0], sx[1])])

    def st_copy(e):
        return remote(mst, yst.at[e], ss.at[e], sr.at[e], kv_1=(y + e) % NY)

    for e in Y_STEPS:
        st_copy(e).start()
    hand_up(0)
    parts = [mst[...]]
    for e in Y_STEPS:
        st_copy(e).wait_recv()
        parts.append(yst[e])
    zst[0] = joined(parts)

    def st_z(d):
        return remote(zst.at[0], zst.at[d], s2.at[d], r2.at[d], kv_0=(z + d) % NZ)

    for d in FAR_FIRST:
        st_z(d).start()
    finished(1)
    vnew[...] = turn[1].astype(BF16).reshape(32, 2, 2, 128)
    go_up(1)
    for s in range(2):
        rows = slice(s * 16, (s + 1) * 16)
        values = jnp.concatenate([kvown[rows, 512:768], kvown[rows, 768:1024]], axis=0)
        accx[s] = contract(weights[s], values, ((0,), (0,))).astype(BF16)
    hand_over(0)
    row = lax.broadcasted_iota(jnp.int32, (128, 128), 0)
    lane = lax.broadcasted_iota(jnp.int32, (128, 128), 1)
    same = row == lane
    lane = lax.broadcasted_iota(jnp.int32, (1, 128), 1) // 16
    lam = jnp.zeros((1, 128), F32)
    for h in range(8):
        lam = jnp.where(lane == h, -lambdas[h], lam)
    for d in Z_STEPS:
        st_z(d).wait_recv()
    gst[...] = joined([zst[d] for d in range(NZ)])

    def b_copy(zc, e):
        to = (y + e) % NY
        return remote(bs.at[to, zc], ybuf.at[e - 1, zc], bss.at[zc, e - 1], bsr.at[zc, e - 1], kv_1=to)

    def send_z(d):
        to = (z + d) % NZ
        return remote(zsum.at[to], zbuf.at[d], zs.at[d], zr.at[d], kv_0=to)

    def mixing(peaks, zc, s):
        ratio = jnp.exp(peaks - gst[zc])
        first = jnp.where(same, ratio[2 * s:2 * s + 1], 0.0)
        second = jnp.where(same, ratio[2 * s + 1:2 * s + 2] * lam, 0.0)
        return jnp.concatenate([first, second], axis=1).astype(BF16)

    def send_blocks(zc, last):
        for s in range(2):
            block = jnp.dot(mixing(st[0, zc], zc, s), acc[zc, s], preferred_element_type=F32)
            if last:
                block += jnp.dot(mixing(sx[0], zc, s), accx[s], preferred_element_type=F32)
            block = block.astype(BF16)
            for i in range(NY):
                bs[i, zc, s] = block[i * 32:(i + 1) * 32]
        for e in Y_STEPS:
            b_copy(zc, e).start()

    def blocks(d, carry):
        send_blocks((z + d) % NZ, False)
        return carry

    lax.fori_loop(1, NZ, blocks, 0)
    send_blocks(z, True)
    def sums(d, carry):
        zc = (z + d) % NZ
        total = bs[y, zc].astype(F32)
        for e in Y_STEPS:
            b_copy(zc, e).wait_recv()
            total += ybuf[e - 1, zc].astype(F32)
        zsum[zc] = total.astype(BF16)

        @pl.when(d < NZ)
        def _():
            send_z(d).start()

        return carry

    lax.fori_loop(1, NZ + 1, sums, 0)
    hand_up(1)
    total = zsum[z].astype(F32)
    for d in range(1, NZ):
        send_z(d).wait_recv()
        total += zbuf[d].astype(F32)
    norm = total * lax.rsqrt(jnp.mean(total * total, axis=-1, keepdims=True) + 1e-05)
    mg[z, y] = (norm * sub[...].astype(F32).reshape(1, 256) * LAMBDA_SCALE).astype(BF16)
    m_start, m_hand_on, m_arrived, m_end = gather_2d(mg, z, y, azs, azr, ays, ayr)
    m_start()
    for d in Z_STEPS:
        m_hand_on(d)
    hand_over(1)
    loads[2].wait()
    for k in (0, *Z_STEPS):
        m_arrived(k)
    result = jnp.zeros((256, 128), F32)
    for h in range(8):
        i, k = h // 2, h % 2
        rows = jnp.concatenate(
            [mg[a, i, s, k * 16:(k + 1) * 16] for a in range(NZ) for s in range(2)], axis=0
        )
        result += jnp.dot(rows, wo[h * 256:(h + 1) * 256], preferred_element_type=F32)
    prod[...] = result.astype(BF16)
    swap = remote(prod, got, xs, xr, tp=1 - c)
    swap.start()
    swap.wait()
    result = prod[...].astype(F32) + got[...].astype(F32)
    out[...] = jnp.where(c == 0, result[:, 0:64], result[:, 64:128]).astype(BF16)

    for e in Y_STEPS:
        gain_copy(e).wait_send()
        tok_copy(e).wait_send()
        st_copy(e).wait_send()
        for i in range(4):
            w_copy(i, e).wait_send()
    for d in Z_STEPS:
        for i in range(2):
            q_copy(i, d).wait_send()
        for m in range(2):
            kv_copy(m, d).wait_send()
        st_z(d).wait_send()
        send_z(d).wait_send()

    m_end()
    for m in range(2):
        to_upper(m, lambda copy: copy.wait_send())

    def drain(zc, carry):
        for e in Y_STEPS:
            b_copy(zc, e).wait_send()
        return carry

    lax.fori_loop(0, NZ, drain, 0)

    @pl.when(upper)
    def _():
        for m in range(2):
            for k in (0, *Z_STEPS):
                up_y(m, k, 1).wait_send()
                up_y(m, k, 3).wait_send()
                up_y(m, k, (3, 1)[m]).wait_recv()
                relay(m, k).wait()


def layer(*operands):
    vmem, smem = pl.BlockSpec(memory_space=pltpu.VMEM), pl.BlockSpec(memory_space=pltpu.SMEM)
    anywhere = pl.BlockSpec(memory_space=pltpu.HBM)
    y_pair, z_pair = [DMA((NY,))] * 2, [DMA((NZ,))] * 2
    zy_pair = [DMA((NZ, NY - 1))] * 2
    return pl.pallas_call(
        layer_kernel,
        name="layer",
        out_shape=(
            jax.ShapeDtypeStruct((256, 64), BF16),
            jax.ShapeDtypeStruct((NZ, NY, 32, 4, 128), BF16),
            jax.ShapeDtypeStruct((NZ, NY, 32, 2, 2, 128), BF16),
        ),
        in_specs=[smem] * 3 + [vmem] * 8 + [anywhere] * 3,
        out_specs=(vmem, anywhere, anywhere),
        scratch_shapes=[
            pltpu.VMEM((NY, 256, 128), BF16),
            pltpu.VMEM((NY, 16, 128), BF16),
            pltpu.VMEM((3, NY, 128, 512), BF16),
            pltpu.VMEM((256, 512), BF16),
            pltpu.VMEM((NZ, 32, 384), BF16),
            pltpu.VMEM((NZ, 32, 256), BF16),
            pltpu.VMEM((2, NZ, 32, 512), BF16),
            pltpu.VMEM((NZ, 32, 384), BF16),
            pltpu.VMEM((NZ, 32, 256), BF16),
            pltpu.VMEM((2, NZ, 32, 512), BF16),
            pltpu.VMEM((NZ, NY, 2, 16, 512), BF16),
            pltpu.VMEM((32, 1024), BF16),
            pltpu.VMEM((32, 4, 128), BF16),
            pltpu.VMEM((32, 2, 2, 128), BF16),
            pltpu.VMEM((2, 128, 128), F32),
            pltpu.VMEM((16, 512, 128), BF16),
            pltpu.VMEM((16, 256, 256), BF16),
            pltpu.VMEM((2048, 128), BF16),
            pltpu.VMEM((512, 128), jnp.int32),
            pltpu.VMEM((2, 512, 128), F32),
            pltpu.VMEM((2, NZ, 4, 128), F32),
            pltpu.VMEM((2, 4, 128), F32),
            pltpu.VMEM((NZ, 4, 128), F32),
            pltpu.VMEM((NZ, 2, 256, 256), BF16),
            pltpu.VMEM((2, 256, 256), BF16),
            pltpu.VMEM((NY, NZ, 4, 128), F32),
            pltpu.VMEM((NZ, NZ, 4, 128), F32),
            pltpu.VMEM((NZ, 4, 128), F32),
            pltpu.VMEM((NY, NZ, 2, 32, 256), BF16),
            pltpu.VMEM((NY - 1, NZ, 2, 32, 256), BF16),
            pltpu.VMEM((NZ, 2, 32, 256), BF16),
            pltpu.VMEM((NZ, 2, 32, 256), BF16),
            pltpu.VMEM((NZ, NY, 2, 32, 256), BF16),
            pltpu.VMEM((256, 128), BF16),
            pltpu.VMEM((256, 128), BF16),
            DMA((8,)), DMA((4, NY)), DMA((4, NY)), *y_pair, *y_pair,
            DMA((2, NZ)), DMA((2, NZ)), DMA((2, NZ)), DMA((2, NZ)),
            *z_pair, *zy_pair, DMA((2, NZ)), DMA((2, NZ)), DMA((2, NZ, NY - 1)), DMA((2, NZ, NY - 1)),
            *y_pair, *z_pair, *zy_pair, *z_pair, DMA, DMA,
        ],
        compiler_params=pltpu.CompilerParams(
            collective_id=0, has_side_effects=True, vmem_limit_bytes=56 * 1024 * 1024
        ),
    )(*operands)


def insert_kernel(length, accepted, k_in, v_in, kg, vg, ko, vo, kt, vt, ins, new, outs):
    z, y, _ = places()
    offset = (z * NY + y) * 32

    def group(g):
        return pl.ds(g * 4, 4)

    def load(g):
        return (
            pltpu.make_async_copy(k_in.at[group(g)], kt.at[group(g), 16:48], ins.at[0, g]),
            pltpu.make_async_copy(v_in.at[group(g)], vt.at[group(g), 16:48], ins.at[1, g]),
        )

    def place(b):
        at = pl.ds(jnp.clip(length[b] + accepted[b] - offset + 16, 0, 48), 16)
        rows = pl.ds((b % 2) * 16, 16)
        return [
            pltpu.make_async_copy(kg.at[b // 2, i, rows], kt.at[b, at, i], new.at[0, b, i]) for i in range(NY)
        ] + [
            pltpu.make_async_copy(vg.at[b // 2, i, rows], vt.at[b, at, :, i], new.at[1, b, i]) for i in range(NY)
        ]

    def store(g):
        return (
            pltpu.make_async_copy(kt.at[group(g), 16:48], ko.at[group(g)], outs.at[0, g]),
            pltpu.make_async_copy(vt.at[group(g), 16:48], vo.at[group(g)], outs.at[1, g]),
        )

    def act(copies, name):
        for copy in copies:
            getattr(copy, name)()

    for g in range(4):
        act(load(g), "start")

    @pl.when(z >= NZ // 2)
    def _():
        for g in range(4):
            act(load(g), "wait")
            for b in range(4 * g, 4 * g + 4):
                act(place(b), "start")
        for g in range(4):
            for b in range(4 * g, 4 * g + 4):
                act(place(b), "wait")
            act(store(g), "start")

    @pl.when(z < NZ // 2)
    def _():
        for g in range(4):
            act(load(g), "wait")
            act(store(g), "start")

    for g in range(4):
        act(store(g), "wait")


def insert(length, accepted, keys, values, new_keys, new_values):
    smem, anywhere = pl.BlockSpec(memory_space=pltpu.SMEM), pl.BlockSpec(memory_space=pltpu.HBM)
    return pl.pallas_call(
        insert_kernel,
        name="insert",
        in_specs=[smem] * 2 + [anywhere] * 4,
        out_specs=(anywhere, anywhere),
        scratch_shapes=[
            pltpu.VMEM((16, 64, NY, 4, 128), BF16), pltpu.VMEM((16, 64, 2, NY, 2, 128), BF16),
            DMA((2, 4)), DMA((2, 16, NY)), DMA((2, 4)),
        ],
        out_shape=(
            jax.ShapeDtypeStruct((16, 32, NY, 4, 128), BF16),
            jax.ShapeDtypeStruct((16, 32, 2, NY, 2, 128), BF16),
        ),
        compiler_params=pltpu.CompilerParams(vmem_limit_bytes=62 * 1024 * 1024),
    )(length, accepted, keys, values, new_keys, new_values)


def per_device(tokens, in_gain, query_weight, key_weight, value_weight, out_weight, lambdas, sub_gain,
               key_cache, value_cache, cache_len, accepted, parents):
    frequency = np.float32(10000.0) ** (-np.arange(64, dtype=np.float32) / np.float32(64))
    frequency = jnp.asarray(np.concatenate([frequency, frequency])[None, :])
    output, new_keys, new_values = layer(
        cache_len, accepted, lambdas, parents, tokens.reshape(256, 128), in_gain.reshape(1, 128),
        sub_gain, frequency, query_weight, key_weight, value_weight,
        key_cache.reshape(16, 512, 128), value_cache.reshape(16, 256, 256), out_weight,
    )
    values = value_cache.reshape(16, 32, NY, 2, 2, 128).transpose(0, 1, 4, 2, 3, 5)
    key_out, value_out = insert(
        cache_len, accepted, key_cache.reshape(16, 32, NY, 4, 128), values, new_keys, new_values
    )
    value_out = value_out.transpose(0, 1, 3, 4, 2, 5).reshape(value_cache.shape)
    return output.reshape(16, 16, 64), key_out.reshape(key_cache.shape), value_out


def solution(mesh):
    torus = Mesh(mesh.devices.reshape(mesh.shape["dp"], NZ, NY, mesh.shape["tp"]), ("dp", "kv_0", "kv_1", "tp"))
    placed = (
        P("dp", None, KV), P(KV), P(KV, "tp"), P(KV, "tp"), P(KV, "tp"), P("tp", KV), P("tp"), P(),
        P("dp", KV, "tp", None, None), P("dp", KV, "tp", None), P("dp"), P("dp"), P("dp", None),
    )
    return jax.shard_map(
        per_device, mesh=torus, in_specs=placed,
        out_specs=(P("dp", None, KV_TP), P("dp", KV, "tp", None, None), P("dp", KV, "tp", None)),
        check_vma=False,
    )
```

```python
import functools
import math

import jax
import jax.numpy as jnp
import numpy as np
from jax import lax
from jax.experimental import pallas as pl
from jax.experimental.pallas import tpu as pltpu
from jax.sharding import Mesh
from jax.sharding import PartitionSpec as P

D = 4096
NZ, NY = 8, 4
KV = ("kv_0", "kv_1")
KV_TP = ("kv_0", "kv_1", "tp")
LAMBDA_SCALE = 0.2 + 0.6 * math.exp(-0.6)
NEG_FILL = -1e30
ROOT = 128 ** (-0.5)
F32, BF16 = jnp.float32, jnp.bfloat16
MESH_ID = pl.DeviceIdType.MESH
DMA = pltpu.SemaphoreType.DMA
Z_STEPS = (1, 7, 2, 6, 3, 5, 4)
Y_STEPS = (1, 3, 2)
FAR_FIRST = (4, 3, 5, 2, 6, 1, 7)


def places():
    return lax.axis_index("kv_0"), lax.axis_index("kv_1"), lax.axis_index("tp")


def remote(src, dst, send_sem, recv_sem, **where):
    return pltpu.make_async_remote_copy(
        src_ref=src, dst_ref=dst, send_sem=send_sem, recv_sem=recv_sem,
        device_id=where, device_id_type=MESH_ID,
    )


def greet(z, y, c, with_tp):
    barrier = pltpu.get_barrier_semaphore()
    for d in range(1, NZ):
        pl.semaphore_signal(barrier, inc=1, device_id={"kv_0": (z + d) % NZ}, device_id_type=MESH_ID)
    for d in range(1, NY):
        pl.semaphore_signal(barrier, inc=1, device_id={"kv_1": (y + d) % NY}, device_id_type=MESH_ID)
    if with_tp:
        pl.semaphore_signal(barrier, inc=1, device_id={"tp": 1 - c}, device_id_type=MESH_ID)
    pl.semaphore_wait(barrier, NZ - 1 + NY - 1 + int(with_tp))


def gather_2d(buf, z, y, zs, zr, ys, yr, relayed):
    direct = (1, 3) if relayed else Y_STEPS

    def z_copy(d):
        return remote(buf.at[z, y], buf.at[z, y], zs.at[d], zr.at[d], kv_0=(z + d) % NZ)

    def y_copy(k, e):
        row = (z + NZ - k) % NZ
        return remote(buf.at[row, y], buf.at[row, y], ys.at[k, e - 1], yr.at[k, e - 1], kv_1=(y + e) % NY)

    def y_relay(k, half):
        at, to = (y + (3, 1)[half]) % NY, (y + (1, 3)[half]) % NY
        block = buf.at[(z + NZ - k) % NZ, at, half]
        return remote(block, block, ys.at[k, 1 + 2 * half], yr.at[k, 1 + 2 * half], kv_1=to)

    def start():
        for d in Z_STEPS:
            z_copy(d).start()
        for e in direct:
            y_copy(0, e).start()

    def hand_on(d):
        z_copy(d).wait_recv()
        for e in direct:
            y_copy(d, e).start()

    def arrived(k):
        for e in direct:
            y_copy(k, e).wait_recv()

    def hand_over(k):
        arrived(k)
        for half in range(2):
            y_relay(k, half).start()

    def handed_over(k):
        for half in range(2):
            y_relay(k, half).wait_recv()

    def end():
        for d in Z_STEPS:
            z_copy(d).wait_send()
        for k in (0, *Z_STEPS):
            for e in direct:
                y_copy(k, e).wait_send()
            if relayed:
                for half in range(2):
                    y_relay(k, half).wait_send()

    return start, hand_on, arrived, hand_over, handed_over, end


def contract(a, b, dims):
    return lax.dot_general(a, b, (dims, ((), ())), preferred_element_type=F32)


def layer_kernel(length, accepted, lambdas, parents, tok, gain, sub, freq, wq, wk, wv, keys_in, values_in, wo_in,
                 out, kg, vg,
                 tokg, gaing, wbuf, nrm, pq0, pq1, pkv, zq0, zq1, zkv, qg, kvown, knew, vnew, turn, kc, vc, wo, code, pscr, st, sx, mst, acc, accx,
                 yst, zst, gst, bs, ybuf, zsum, zbuf, mg, prod, got,
                 ls, ws, wr, ts, tr, gs, gr, qs, qr, ks, kr, azs, azr, ays, ayr, kzs, kzr, kys, kyr,
                 ss, sr, s2, r2, bss, bsr, zs, zr, xs, xr):
    z, y, c = places()
    loads = [
        pltpu.make_async_copy(src, dst, ls.at[3 + i])
        for i, (src, dst) in enumerate(((keys_in, kc), (values_in, vc), (wo_in, wo)))
    ]
    gaing[y] = jnp.broadcast_to(gain[...], (16, 128))
    greet(z, y, c, True)
    ws_in = (wq, wk, wv)

    def tok_copy(e):
        return remote(tok, tokg.at[y], ts.at[e], tr.at[e], kv_1=(y + e) % NY)

    def gain_copy(e):
        return remote(gaing.at[y], gaing.at[y], gs.at[e], gr.at[e], kv_1=(y + e) % NY)

    pieces = ((0, 0, 256), (0, 256, 256), (1, 0, 512), (2, 0, 512))

    def w_copy(i, e):
        to = (y + e) % NY
        m, first, size = pieces[i]
        cols = pl.ds(pl.multiple_of(to * 512 + first, 256), size)
        into = wbuf.at[m, y, :, first:first + size]
        return remote(ws_in[m].at[:, cols], into, ws.at[i, e], wr.at[i, e], kv_1=to)

    for e in Y_STEPS:
        gain_copy(e).start()
        tok_copy(e).start()
    for i in range(4):
        for e in Y_STEPS:
            w_copy(i, e).start()
    mine = pl.ds(pl.multiple_of(y * 512, 512), 512)
    own = [pltpu.make_async_copy(ws_in[m].at[:, mine], wbuf.at[m, y], ls.at[m]) for m in range(3)]
    for o in own:
        o.start()
    for load in loads:
        load.start()
    tokg[y] = tok[...]

    row16 = lax.broadcasted_iota(jnp.int32, (16, 16), 0)
    lane16 = lax.broadcasted_iota(jnp.int32, (16, 16), 1)
    unit = (row16 == lane16).astype(F32)
    spread16 = (lax.broadcasted_iota(jnp.int32, (16, 128), 1) % 16 == lax.broadcasted_iota(jnp.int32, (16, 128), 0)).astype(BF16)
    near = parents[pl.ds(2 * z, 2), :]
    seen, angles = [], []
    for s in range(2):
        reach = jnp.maximum(unit, (near[s:s + 1, :] == row16).astype(F32))
        for _ in range(4):
            half = reach.astype(BF16)
            reach = jnp.minimum(jnp.dot(half, half, preferred_element_type=F32), 1.0)
        half = reach.astype(BF16)
        seen.append(jnp.dot(half, spread16, preferred_element_type=F32))
        depth = contract(half, jnp.ones((16, 128), BF16), ((0,), (0,))) - 1.0
        begin = length[2 * z + s] + accepted[2 * z + s]
        angles.append((begin.astype(F32) + depth) * freq[...])
    angle = jnp.concatenate(angles, axis=0)
    cos = jnp.cos(angle)
    sin = jnp.where(lax.broadcasted_iota(jnp.int32, (32, 128), 1) < 64, -1.0, 1.0) * jnp.sin(angle)
    row = lax.broadcasted_iota(jnp.int32, (512, 128), 0)
    lane = lax.broadcasted_iota(jnp.int32, (512, 128), 1)
    code[...] = jnp.where(((row // 2) % 8) == (lane // 16), row // 16, 4096)

    for e in Y_STEPS:
        gain_copy(e).wait_recv()
        tok_copy(e).wait_recv()
    power = jnp.zeros((256, 1), F32)
    for a in range(NY):
        wide = tokg[a].astype(F32)
        power += jnp.sum(wide * wide, axis=-1, keepdims=True)
        nrm[:, a * 128:(a + 1) * 128] = (wide * gaing[a, 0:1].astype(F32)).astype(BF16)
    high = power.astype(BF16)
    rest = power - high.astype(F32)
    mid = rest.astype(BF16)
    low = (rest - mid.astype(F32)).astype(BF16)
    lane = lax.broadcasted_iota(jnp.int32, (256, 128), 1)
    terms = jnp.where(lane == 0, high.astype(F32), jnp.where(lane == 1, mid.astype(F32), low.astype(F32)))
    terms = jnp.where(lane < 3, terms, 0.0)
    pq0[:, :, 256:384] = terms.astype(BF16).reshape(NZ, 32, 128)

    def product(i):
        m, first, size = pieces[i]
        if first == 0:
            own[m].wait()
        for e in Y_STEPS:
            w_copy(i, e).wait_recv()
        total = jnp.zeros((256, size), F32)
        for a in range(NY):
            total += jnp.dot(
                nrm[:, a * 128:(a + 1) * 128], wbuf[m, a, :, first:first + size], preferred_element_type=F32
            )
        return total.astype(BF16).reshape(NZ, 32, size)

    halves = ((pq0, zq0), (pq1, zq1))

    def q_copy(i, d):
        to = (z + d) % NZ
        return remote(halves[i][0].at[to], halves[i][1].at[d], qs.at[i, d], qr.at[i, d], kv_0=to)

    def kv_copy(m, d):
        to = (z + d) % NZ
        return remote(pkv.at[m, to], zkv.at[m, d], ks.at[m, d], kr.at[m, d], kv_0=to)

    pq0[:, :, 0:256] = product(0)
    for d in FAR_FIRST:
        q_copy(0, d).start()
    pq1[...] = product(1)
    for d in FAR_FIRST:
        q_copy(1, d).start()
    pkv[0] = product(2)
    for d in FAR_FIRST:
        kv_copy(0, d).start()

    totals = []
    for i in range(2):
        total = halves[i][0][z].astype(F32)
        for d in Z_STEPS:
            q_copy(i, d).wait_recv()
            total += halves[i][1][d].astype(F32)
        totals.append(total)
    power = jnp.sum(totals[0][:, 256:384], axis=-1, keepdims=True)
    scale = lax.rsqrt(power / D + 1e-06)

    def turned(block):
        return block * cos + pltpu.roll(block, 64, 1) * sin

    for v in range(4):
        cols = slice(v * 128, (v + 1) * 128)
        block = turned(totals[v // 2][:, v % 2 * 128:v % 2 * 128 + 128] * scale).astype(BF16)
        qg[z, y, 0, :, cols] = block[0:16]
        qg[z, y, 1, :, cols] = block[16:32]
    q_start, q_hand_on, q_arrived, _, _, q_end = gather_2d(qg, z, y, azs, azr, ays, ayr, False)
    q_start()
    def finished(m):
        total = pkv[m, z].astype(F32)
        for d in Z_STEPS:
            kv_copy(m, d).wait_recv()
            total += zkv[m, d].astype(F32)
        for v in range(4):
            block = total[:, v * 128:(v + 1) * 128] * scale
            if m == 0:
                block = turned(block)
            at = m * 512 + v * 128
            kvown[:, at:at + 128] = block.astype(BF16)
            turn[m, pl.ds((v % 2) * 2 + v // 2 if m else v, 32, stride=4), :] = block

    upper = z >= NZ // 2

    pairs = ((knew, kg), (vnew, vg))

    def up_z(m, d):
        return remote(pairs[m][0], pairs[m][1].at[z, y], kzs.at[m, d], kzr.at[m, d], kv_0=(z + d) % NZ)

    def up_y(m, k, e):
        block = pairs[m][1].at[(z + NZ - k) % NZ, y]
        return remote(block, block, kys.at[m, k, e - 1], kyr.at[m, k, e - 1], kv_1=(y + e) % NY)

    own_up = [pltpu.make_async_copy(pairs[m][0], pairs[m][1].at[z, y], ls.at[6 + m]) for m in range(2)]

    def relay(m, k):
        at, to = (z + NZ - k) % NZ, (y + (1, 3)[k % 2]) % NY
        block = pairs[m][1].at[at, (y + (3, 1)[k % 2]) % NY]
        return remote(block, block, kys.at[m, k, 1], kyr.at[m, k, 1], kv_1=to)

    def to_upper(m, act):
        for d in Z_STEPS:
            @pl.when((z + d) % NZ >= NZ // 2)
            def _():
                act(up_z(m, d))

    def go_up(m):
        to_upper(m, lambda copy: copy.start())

        @pl.when(upper)
        def _():
            own_up[m].start()

    def hand_up(m):
        @pl.when(upper)
        def _():
            own_up[m].wait()
            for k in (0, *Z_STEPS):
                if k:
                    up_z(m, k).wait_recv()
                for e in (1, 3):
                    up_y(m, k, e).start()

    def hand_over(m):
        @pl.when(upper)
        def _():
            for k in (0, *Z_STEPS):
                up_y(m, k, (1, 3)[k % 2]).wait_recv()
                relay(m, k).start()

    def queries_of(zc, s):
        return jnp.concatenate(
            [qg[zc, i, s, :, (h * 2 + m) * 128:(h * 2 + m + 1) * 128] for m in range(2) for i in range(NY) for h in range(2)],
            axis=0,
        )

    odd = lax.broadcasted_iota(jnp.int32, (8, 128), 0) % 2 == 1
    offset = (z * NY + y) * 32

    def nth(step):
        return jnp.where(step % 2 == 1, (step + 1) // 2, (NZ - step // 2) % NZ)

    def attend(step, carry):
        k = nth(step)
        q_arrived(k)
        zc = (z + NZ - k) % NZ
        for s in range(2):
            b = 2 * zc + s
            limit = length[b] + accepted[b] - offset
            both = contract(kc[b], queries_of(zc, s), ((1,), (1,)))
            both = both.reshape(64, 8, 256)
            live = (code[...] < limit).reshape(64, 8, 128)
            score = jnp.where(odd[None], both[:, :, 128:], both[:, :, :128]) * ROOT
            score = jnp.where(live, score, NEG_FILL)
            top = jnp.max(score, axis=0)
            peaks = [jnp.max(jnp.where(odd == bool(m), top, NEG_FILL), axis=0, keepdims=True) for m in range(2)]
            peak = jnp.where(odd, peaks[1], peaks[0])
            grown = jnp.where(live, jnp.exp(score - peak[None]), 0.0)
            part = jnp.sum(grown, axis=0)
            for m in range(2):
                st[0, zc, 2 * s + m:2 * s + m + 1] = peaks[m]
                st[1, zc, 2 * s + m:2 * s + m + 1] = jnp.sum(jnp.where(odd == bool(m), part, 0.0), axis=0, keepdims=True)
            pscr[s] = grown.reshape(512, 128)
            chance = jnp.concatenate([pscr[s, pl.ds(m, 256, stride=2), :] for m in range(2)], axis=1).astype(BF16)
            acc[zc, s] = contract(chance, vc[b], ((0,), (0,))).astype(BF16)
        return carry

    for d in Z_STEPS[:4]:
        q_hand_on(d)
    loads[0].wait()
    loads[1].wait()
    attend(jnp.int32(0), 0)
    for d in Z_STEPS[4:]:
        q_hand_on(d)
    finished(0)
    knew[...] = turn[0].astype(BF16).reshape(32, 4, 128)
    go_up(0)
    pkv[1] = product(3)
    for d in Z_STEPS:
        kv_copy(1, d).start()

    lax.fori_loop(1, NZ, attend, 0)
    q_end()

    weights = []
    head_row = 2 * y + lax.broadcasted_iota(jnp.int32, (32, 128), 0) // 16
    head_lane = lax.broadcasted_iota(jnp.int32, (32, 128), 1) // 16
    for s in range(2):
        rows = slice(s * 16, (s + 1) * 16)
        keys = jnp.concatenate(
            [kvown[rows, (h * 2 + m) * 128:(h * 2 + m + 1) * 128] for m in range(2) for h in range(2)], axis=0
        )
        both = contract(keys, queries_of(z, s), ((1,), (1,)))
        live = (head_row == head_lane) & (jnp.concatenate([seen[s], seen[s]], axis=0) > 0.5)
        chance = []
        for m in range(2):
            score = jnp.where(live, both[m * 32:(m + 1) * 32, m * 128:(m + 1) * 128] * ROOT, NEG_FILL)
            peak = jnp.max(score, axis=0, keepdims=True)
            grown = jnp.where(live, jnp.exp(score - peak), 0.0)
            sx[0, 2 * s + m:2 * s + m + 1] = peak
            sx[1, 2 * s + m:2 * s + m + 1] = jnp.sum(grown, axis=0, keepdims=True)
            chance.append(grown)
        weights.append(jnp.concatenate(chance, axis=1).astype(BF16))
    def log_sum(peak, total):
        return peak + jnp.log(jnp.maximum(total, 1e-30))

    def joined(parts):
        peak = functools.reduce(jnp.maximum, parts)
        return log_sum(peak, sum(jnp.exp(part - peak) for part in parts))

    mst[...] = log_sum(st[0], st[1])
    mst[z] = joined([mst[z], log_sum(sx[0], sx[1])])

    def st_copy(e):
        return remote(mst, yst.at[e], ss.at[e], sr.at[e], kv_1=(y + e) % NY)

    for e in Y_STEPS:
        st_copy(e).start()
    hand_up(0)
    parts = [mst[...]]
    for e in Y_STEPS:
        st_copy(e).wait_recv()
        parts.append(yst[e])
    zst[0] = joined(parts)

    def st_z(d):
        return remote(zst.at[0], zst.at[d], s2.at[d], r2.at[d], kv_0=(z + d) % NZ)

    for d in FAR_FIRST:
        st_z(d).start()
    finished(1)
    vnew[...] = turn[1].astype(BF16).reshape(32, 2, 2, 128)
    go_up(1)
    for s in range(2):
        rows = slice(s * 16, (s + 1) * 16)
        values = jnp.concatenate([kvown[rows, 512:768], kvown[rows, 768:1024]], axis=0)
        accx[s] = contract(weights[s], values, ((0,), (0,))).astype(BF16)
    hand_over(0)
    row = lax.broadcasted_iota(jnp.int32, (128, 128), 0)
    lane = lax.broadcasted_iota(jnp.int32, (128, 128), 1)
    same = row == lane
    lane = lax.broadcasted_iota(jnp.int32, (1, 128), 1) // 16
    lam = jnp.zeros((1, 128), F32)
    for h in range(8):
        lam = jnp.where(lane == h, -lambdas[h], lam)
    for d in Z_STEPS:
        st_z(d).wait_recv()
    gst[...] = joined([zst[d] for d in range(NZ)])

    def b_copy(zc, e):
        to = (y + e) % NY
        return remote(bs.at[to, zc], ybuf.at[e - 1, zc], bss.at[zc, e - 1], bsr.at[zc, e - 1], kv_1=to)

    def send_z(d):
        to = (z + d) % NZ
        return remote(zsum.at[to], zbuf.at[d], zs.at[d], zr.at[d], kv_0=to)

    def mixing(peaks, zc, s):
        ratio = jnp.exp(peaks - gst[zc])
        first = jnp.where(same, ratio[2 * s:2 * s + 1], 0.0)
        second = jnp.where(same, ratio[2 * s + 1:2 * s + 2] * lam, 0.0)
        return jnp.concatenate([first, second], axis=1).astype(BF16)

    def send_blocks(zc, last):
        for s in range(2):
            block = jnp.dot(mixing(st[0, zc], zc, s), acc[zc, s], preferred_element_type=F32)
            if last:
                block += jnp.dot(mixing(sx[0], zc, s), accx[s], preferred_element_type=F32)
            block = block.astype(BF16)
            for i in range(NY):
                bs[i, zc, s] = block[i * 32:(i + 1) * 32]
        for e in Y_STEPS:
            b_copy(zc, e).start()

    def blocks(d, carry):
        send_blocks((z + d) % NZ, False)
        return carry

    lax.fori_loop(1, NZ, blocks, 0)
    send_blocks(z, True)
    def sums(d, carry):
        zc = (z + d) % NZ
        total = bs[y, zc].astype(F32)
        for e in Y_STEPS:
            b_copy(zc, e).wait_recv()
            total += ybuf[e - 1, zc].astype(F32)
        zsum[zc] = total.astype(BF16)

        @pl.when(d < NZ)
        def _():
            send_z(d).start()

        return carry

    lax.fori_loop(1, NZ + 1, sums, 0)
    hand_up(1)
    total = zsum[z].astype(F32)
    for d in range(1, NZ):
        send_z(d).wait_recv()
        total += zbuf[d].astype(F32)
    norm = total * lax.rsqrt(jnp.mean(total * total, axis=-1, keepdims=True) + 1e-05)
    mg[z, y] = (norm * sub[...].astype(F32).reshape(1, 256) * LAMBDA_SCALE).astype(BF16)
    m_start, m_hand_on, m_arrived, _, _, m_end = gather_2d(mg, z, y, azs, azr, ays, ayr, False)
    r_start, r_hand_on, _, r_hand_over, r_handed_over, r_end = gather_2d(mg, z, y, azs, azr, ays, ayr, True)
    @pl.when(upper)
    def _():
        r_start()
        for d in Z_STEPS:
            r_hand_on(d)
        for k in (0, *Z_STEPS):
            r_hand_over(k)

    @pl.when(z < NZ // 2)
    def _():
        m_start()
        for d in Z_STEPS:
            m_hand_on(d)

    hand_over(1)
    loads[2].wait()

    @pl.when(upper)
    def _():
        for k in (0, *Z_STEPS):
            r_handed_over(k)

    @pl.when(z < NZ // 2)
    def _():
        for k in (0, *Z_STEPS):
            m_arrived(k)

    result = jnp.zeros((256, 128), F32)
    for h in range(8):
        i, k = h // 2, h % 2
        rows = jnp.concatenate(
            [mg[a, i, s, k * 16:(k + 1) * 16] for a in range(NZ) for s in range(2)], axis=0
        )
        result += jnp.dot(rows, wo[h * 256:(h + 1) * 256], preferred_element_type=F32)
    prod[...] = result.astype(BF16)
    swap = remote(prod, got, xs, xr, tp=1 - c)
    swap.start()
    swap.wait()
    result = prod[...].astype(F32) + got[...].astype(F32)
    out[...] = jnp.where(c == 0, result[:, 0:64], result[:, 64:128]).astype(BF16)

    for e in Y_STEPS:
        gain_copy(e).wait_send()
        tok_copy(e).wait_send()
        st_copy(e).wait_send()
        for i in range(4):
            w_copy(i, e).wait_send()
    for d in Z_STEPS:
        for i in range(2):
            q_copy(i, d).wait_send()
        for m in range(2):
            kv_copy(m, d).wait_send()
        st_z(d).wait_send()
        send_z(d).wait_send()

    pl.when(upper)(r_end)
    pl.when(z < NZ // 2)(m_end)
    for m in range(2):
        to_upper(m, lambda copy: copy.wait_send())

    def drain(zc, carry):
        for e in Y_STEPS:
            b_copy(zc, e).wait_send()
        return carry

    lax.fori_loop(0, NZ, drain, 0)

    @pl.when(upper)
    def _():
        for m in range(2):
            for k in (0, *Z_STEPS):
                up_y(m, k, 1).wait_send()
                up_y(m, k, 3).wait_send()
                up_y(m, k, (3, 1)[k % 2]).wait_recv()
                relay(m, k).wait()


def layer(*operands):
    vmem, smem = pl.BlockSpec(memory_space=pltpu.VMEM), pl.BlockSpec(memory_space=pltpu.SMEM)
    anywhere = pl.BlockSpec(memory_space=pltpu.HBM)
    y_pair, z_pair = [DMA((NY,))] * 2, [DMA((NZ,))] * 2
    zy_pair = [DMA((NZ, NY - 1))] * 2
    return pl.pallas_call(
        layer_kernel,
        name="layer",
        out_shape=(
            jax.ShapeDtypeStruct((256, 64), BF16),
            jax.ShapeDtypeStruct((NZ, NY, 32, 4, 128), BF16),
            jax.ShapeDtypeStruct((NZ, NY, 32, 2, 2, 128), BF16),
        ),
        in_specs=[smem] * 3 + [vmem] * 8 + [anywhere] * 3,
        out_specs=(vmem, anywhere, anywhere),
        scratch_shapes=[
            pltpu.VMEM((NY, 256, 128), BF16),
            pltpu.VMEM((NY, 16, 128), BF16),
            pltpu.VMEM((3, NY, 128, 512), BF16),
            pltpu.VMEM((256, 512), BF16),
            pltpu.VMEM((NZ, 32, 384), BF16),
            pltpu.VMEM((NZ, 32, 256), BF16),
            pltpu.VMEM((2, NZ, 32, 512), BF16),
            pltpu.VMEM((NZ, 32, 384), BF16),
            pltpu.VMEM((NZ, 32, 256), BF16),
            pltpu.VMEM((2, NZ, 32, 512), BF16),
            pltpu.VMEM((NZ, NY, 2, 16, 512), BF16),
            pltpu.VMEM((32, 1024), BF16),
            pltpu.VMEM((32, 4, 128), BF16),
            pltpu.VMEM((32, 2, 2, 128), BF16),
            pltpu.VMEM((2, 128, 128), F32),
            pltpu.VMEM((16, 512, 128), BF16),
            pltpu.VMEM((16, 256, 256), BF16),
            pltpu.VMEM((2048, 128), BF16),
            pltpu.VMEM((512, 128), jnp.int32),
            pltpu.VMEM((2, 512, 128), F32),
            pltpu.VMEM((2, NZ, 4, 128), F32),
            pltpu.VMEM((2, 4, 128), F32),
            pltpu.VMEM((NZ, 4, 128), F32),
            pltpu.VMEM((NZ, 2, 256, 256), BF16),
            pltpu.VMEM((2, 256, 256), BF16),
            pltpu.VMEM((NY, NZ, 4, 128), F32),
            pltpu.VMEM((NZ, NZ, 4, 128), F32),
            pltpu.VMEM((NZ, 4, 128), F32),
            pltpu.VMEM((NY, NZ, 2, 32, 256), BF16),
            pltpu.VMEM((NY - 1, NZ, 2, 32, 256), BF16),
            pltpu.VMEM((NZ, 2, 32, 256), BF16),
            pltpu.VMEM((NZ, 2, 32, 256), BF16),
            pltpu.VMEM((NZ, NY, 2, 32, 256), BF16),
            pltpu.VMEM((256, 128), BF16),
            pltpu.VMEM((256, 128), BF16),
            DMA((8,)), DMA((4, NY)), DMA((4, NY)), *y_pair, *y_pair,
            DMA((2, NZ)), DMA((2, NZ)), DMA((2, NZ)), DMA((2, NZ)),
            *z_pair, DMA((NZ, NY)), DMA((NZ, NY)), DMA((2, NZ)), DMA((2, NZ)), DMA((2, NZ, NY - 1)), DMA((2, NZ, NY - 1)),
            *y_pair, *z_pair, *zy_pair, *z_pair, DMA, DMA,
        ],
        compiler_params=pltpu.CompilerParams(
            collective_id=0, has_side_effects=True, vmem_limit_bytes=56 * 1024 * 1024
        ),
    )(*operands)


def insert_kernel(length, accepted, k_in, v_in, kg, vg, ko, vo, kt, vt, ins, new, outs):
    z, y, _ = places()
    offset = (z * NY + y) * 32

    def group(g):
        return pl.ds(g * 4, 4)

    def load(g):
        return (
            pltpu.make_async_copy(k_in.at[group(g)], kt.at[group(g), 16:48], ins.at[0, g]),
            pltpu.make_async_copy(v_in.at[group(g)], vt.at[group(g), 16:48], ins.at[1, g]),
        )

    def place(b):
        at = pl.ds(jnp.clip(length[b] + accepted[b] - offset + 16, 0, 48), 16)
        rows = pl.ds((b % 2) * 16, 16)
        return [
            pltpu.make_async_copy(kg.at[b // 2, i, rows], kt.at[b, at, i], new.at[0, b, i]) for i in range(NY)
        ] + [
            pltpu.make_async_copy(vg.at[b // 2, i, rows], vt.at[b, at, :, i], new.at[1, b, i]) for i in range(NY)
        ]

    def store(g):
        return (
            pltpu.make_async_copy(kt.at[group(g), 16:48], ko.at[group(g)], outs.at[0, g]),
            pltpu.make_async_copy(vt.at[group(g), 16:48], vo.at[group(g)], outs.at[1, g]),
        )

    def act(copies, name):
        for copy in copies:
            getattr(copy, name)()

    for g in range(4):
        act(load(g), "start")

    @pl.when(z >= NZ // 2)
    def _():
        for g in range(4):
            act(load(g), "wait")
            for b in range(4 * g, 4 * g + 4):
                act(place(b), "start")
        for g in range(4):
            for b in range(4 * g, 4 * g + 4):
                act(place(b), "wait")
            act(store(g), "start")

    @pl.when(z < NZ // 2)
    def _():
        for g in range(4):
            act(load(g), "wait")
            act(store(g), "start")

    for g in range(4):
        act(store(g), "wait")


def insert(length, accepted, keys, values, new_keys, new_values):
    smem, anywhere = pl.BlockSpec(memory_space=pltpu.SMEM), pl.BlockSpec(memory_space=pltpu.HBM)
    return pl.pallas_call(
        insert_kernel,
        name="insert",
        in_specs=[smem] * 2 + [anywhere] * 4,
        out_specs=(anywhere, anywhere),
        scratch_shapes=[
            pltpu.VMEM((16, 64, NY, 4, 128), BF16), pltpu.VMEM((16, 64, 2, NY, 2, 128), BF16),
            DMA((2, 4)), DMA((2, 16, NY)), DMA((2, 4)),
        ],
        out_shape=(
            jax.ShapeDtypeStruct((16, 32, NY, 4, 128), BF16),
            jax.ShapeDtypeStruct((16, 32, 2, NY, 2, 128), BF16),
        ),
        compiler_params=pltpu.CompilerParams(vmem_limit_bytes=62 * 1024 * 1024),
    )(length, accepted, keys, values, new_keys, new_values)


def per_device(tokens, in_gain, query_weight, key_weight, value_weight, out_weight, lambdas, sub_gain,
               key_cache, value_cache, cache_len, accepted, parents):
    frequency = np.float32(10000.0) ** (-np.arange(64, dtype=np.float32) / np.float32(64))
    frequency = jnp.asarray(np.concatenate([frequency, frequency])[None, :])
    output, new_keys, new_values = layer(
        cache_len, accepted, lambdas, parents, tokens.reshape(256, 128), in_gain.reshape(1, 128),
        sub_gain, frequency, query_weight, key_weight, value_weight,
        key_cache.reshape(16, 512, 128), value_cache.reshape(16, 256, 256), out_weight,
    )
    values = value_cache.reshape(16, 32, NY, 2, 2, 128).transpose(0, 1, 4, 2, 3, 5)
    key_out, value_out = insert(
        cache_len, accepted, key_cache.reshape(16, 32, NY, 4, 128), values, new_keys, new_values
    )
    value_out = value_out.transpose(0, 1, 3, 4, 2, 5).reshape(value_cache.shape)
    return output.reshape(16, 16, 64), key_out.reshape(key_cache.shape), value_out


def solution(mesh):
    torus = Mesh(mesh.devices.reshape(mesh.shape["dp"], NZ, NY, mesh.shape["tp"]), ("dp", "kv_0", "kv_1", "tp"))
    placed = (
        P("dp", None, KV), P(KV), P(KV, "tp"), P(KV, "tp"), P(KV, "tp"), P("tp", KV), P("tp"), P(),
        P("dp", KV, "tp", None, None), P("dp", KV, "tp", None), P("dp"), P("dp"), P("dp", None),
    )
    return jax.shard_map(
        per_device, mesh=torus, in_specs=placed,
        out_specs=(P("dp", None, KV_TP), P("dp", KV, "tp", None, None), P("dp", KV, "tp", None)),
        check_vma=False,
    )
```

```python
import functools
import math

import jax
import jax.numpy as jnp
import numpy as np
from jax import lax
from jax.experimental import pallas as pl
from jax.experimental.pallas import tpu as pltpu
from jax.sharding import Mesh
from jax.sharding import PartitionSpec as P

D = 4096
NZ, NY = 8, 4
KV = ("kv_0", "kv_1")
KV_TP = ("kv_0", "kv_1", "tp")
LAMBDA_SCALE = 0.2 + 0.6 * math.exp(-0.6)
NEG_FILL = -1e30
ROOT = 128 ** (-0.5)
F32, BF16 = jnp.float32, jnp.bfloat16
MESH_ID = pl.DeviceIdType.MESH
DMA = pltpu.SemaphoreType.DMA
Z_STEPS = (1, 7, 2, 6, 3, 5, 4)
Y_STEPS = (1, 3, 2)
FAR_FIRST = (4, 3, 5, 2, 6, 1, 7)


def places():
    return lax.axis_index("kv_0"), lax.axis_index("kv_1"), lax.axis_index("tp")


def remote(src, dst, send_sem, recv_sem, **where):
    return pltpu.make_async_remote_copy(
        src_ref=src, dst_ref=dst, send_sem=send_sem, recv_sem=recv_sem,
        device_id=where, device_id_type=MESH_ID,
    )


def greet(z, y, c, with_tp):
    barrier = pltpu.get_barrier_semaphore()
    for d in range(1, NZ):
        pl.semaphore_signal(barrier, inc=1, device_id={"kv_0": (z + d) % NZ}, device_id_type=MESH_ID)
    for d in range(1, NY):
        pl.semaphore_signal(barrier, inc=1, device_id={"kv_1": (y + d) % NY}, device_id_type=MESH_ID)
    if with_tp:
        pl.semaphore_signal(barrier, inc=1, device_id={"tp": 1 - c}, device_id_type=MESH_ID)
    pl.semaphore_wait(barrier, NZ - 1 + NY - 1 + int(with_tp))


def gather_2d(buf, z, y, zs, zr, ys, yr, relayed):
    direct = (1, 3) if relayed else Y_STEPS

    def z_copy(d):
        return remote(buf.at[z, y], buf.at[z, y], zs.at[d], zr.at[d], kv_0=(z + d) % NZ)

    def y_copy(k, e):
        row = (z + NZ - k) % NZ
        return remote(buf.at[row, y], buf.at[row, y], ys.at[k, e - 1], yr.at[k, e - 1], kv_1=(y + e) % NY)

    def y_relay(k, half):
        at, to = (y + (3, 1)[half]) % NY, (y + (1, 3)[half]) % NY
        block = buf.at[(z + NZ - k) % NZ, at, half]
        return remote(block, block, ys.at[k, 1 + 2 * half], yr.at[k, 1 + 2 * half], kv_1=to)

    def start(steps=Z_STEPS, along_y=True):
        for d in steps:
            z_copy(d).start()
        if along_y:
            for e in direct:
                y_copy(0, e).start()

    def hand_on(d):
        z_copy(d).wait_recv()
        for e in direct:
            y_copy(d, e).start()

    def arrived(k):
        for e in direct:
            y_copy(k, e).wait_recv()

    def hand_over(k):
        arrived(k)
        for half in range(2):
            y_relay(k, half).start()

    def handed_over(k):
        for half in range(2):
            y_relay(k, half).wait_recv()

    def end():
        for d in Z_STEPS:
            z_copy(d).wait_send()
        for k in (0, *Z_STEPS):
            for e in direct:
                y_copy(k, e).wait_send()
            if relayed:
                for half in range(2):
                    y_relay(k, half).wait_send()

    return start, hand_on, arrived, hand_over, handed_over, end


def contract(a, b, dims):
    return lax.dot_general(a, b, (dims, ((), ())), preferred_element_type=F32)


def layer_kernel(length, accepted, lambdas, parents, tok, gain, sub, freq, wq, wk, wv, keys_in, values_in, wo_in,
                 out, kg, vg,
                 tokg, gaing, wbuf, nrm, pq0, pq1, pkv, zq0, zq1, zkv, qg, kvown, knew, vnew, turn, kc, vc, wo, code, pscr, st, sx, mst, acc, accx,
                 yst, zst, gst, bs, ybuf, zsum, zbuf, mg, prod, got,
                 ls, ws, wr, ts, tr, gs, gr, qs, qr, ks, kr, azs, azr, ays, ayr, kzs, kzr, kys, kyr,
                 ss, sr, s2, r2, bss, bsr, zs, zr, xs, xr):
    z, y, c = places()
    loads = [
        pltpu.make_async_copy(src, dst, ls.at[3 + i])
        for i, (src, dst) in enumerate(((keys_in, kc), (values_in, vc), (wo_in, wo)))
    ]
    gaing[y] = jnp.broadcast_to(gain[...], (16, 128))
    greet(z, y, c, True)
    ws_in = (wq, wk, wv)

    def tok_copy(e):
        return remote(tok, tokg.at[y], ts.at[e], tr.at[e], kv_1=(y + e) % NY)

    def gain_copy(e):
        return remote(gaing.at[y], gaing.at[y], gs.at[e], gr.at[e], kv_1=(y + e) % NY)

    pieces = ((0, 0, 256), (0, 256, 256), (1, 0, 512), (2, 0, 512))

    def w_copy(i, e):
        to = (y + e) % NY
        m, first, size = pieces[i]
        cols = pl.ds(pl.multiple_of(to * 512 + first, 256), size)
        into = wbuf.at[m, y, :, first:first + size]
        return remote(ws_in[m].at[:, cols], into, ws.at[i, e], wr.at[i, e], kv_1=to)

    for e in Y_STEPS:
        gain_copy(e).start()
        tok_copy(e).start()
    for i in range(4):
        for e in Y_STEPS:
            w_copy(i, e).start()
    mine = pl.ds(pl.multiple_of(y * 512, 512), 512)
    own = [pltpu.make_async_copy(ws_in[m].at[:, mine], wbuf.at[m, y], ls.at[m]) for m in range(3)]
    for o in own:
        o.start()
    for load in loads:
        load.start()
    tokg[y] = tok[...]

    row16 = lax.broadcasted_iota(jnp.int32, (16, 16), 0)
    lane16 = lax.broadcasted_iota(jnp.int32, (16, 16), 1)
    unit = (row16 == lane16).astype(F32)
    spread16 = (lax.broadcasted_iota(jnp.int32, (16, 128), 1) % 16 == lax.broadcasted_iota(jnp.int32, (16, 128), 0)).astype(BF16)
    near = parents[pl.ds(2 * z, 2), :]
    seen, angles = [], []
    for s in range(2):
        reach = jnp.maximum(unit, (near[s:s + 1, :] == row16).astype(F32))
        for _ in range(4):
            half = reach.astype(BF16)
            reach = jnp.minimum(jnp.dot(half, half, preferred_element_type=F32), 1.0)
        half = reach.astype(BF16)
        seen.append(jnp.dot(half, spread16, preferred_element_type=F32))
        depth = contract(half, jnp.ones((16, 128), BF16), ((0,), (0,))) - 1.0
        begin = length[2 * z + s] + accepted[2 * z + s]
        angles.append((begin.astype(F32) + depth) * freq[...])
    angle = jnp.concatenate(angles, axis=0)
    cos = jnp.cos(angle)
    sin = jnp.where(lax.broadcasted_iota(jnp.int32, (32, 128), 1) < 64, -1.0, 1.0) * jnp.sin(angle)
    row = lax.broadcasted_iota(jnp.int32, (512, 128), 0)
    lane = lax.broadcasted_iota(jnp.int32, (512, 128), 1)
    code[...] = jnp.where(((row // 2) % 8) == (lane // 16), row // 16, 4096)

    for e in Y_STEPS:
        gain_copy(e).wait_recv()
        tok_copy(e).wait_recv()
    power = jnp.zeros((256, 1), F32)
    for a in range(NY):
        wide = tokg[a].astype(F32)
        power += jnp.sum(wide * wide, axis=-1, keepdims=True)
        nrm[:, a * 128:(a + 1) * 128] = (wide * gaing[a, 0:1].astype(F32)).astype(BF16)
    high = power.astype(BF16)
    rest = power - high.astype(F32)
    mid = rest.astype(BF16)
    low = (rest - mid.astype(F32)).astype(BF16)
    lane = lax.broadcasted_iota(jnp.int32, (256, 128), 1)
    terms = jnp.where(lane == 0, high.astype(F32), jnp.where(lane == 1, mid.astype(F32), low.astype(F32)))
    terms = jnp.where(lane < 3, terms, 0.0)
    pq0[:, :, 256:384] = terms.astype(BF16).reshape(NZ, 32, 128)

    def product(i):
        m, first, size = pieces[i]
        if first == 0:
            own[m].wait()
        for e in Y_STEPS:
            w_copy(i, e).wait_recv()
        total = jnp.zeros((256, size), F32)
        for a in range(NY):
            total += jnp.dot(
                nrm[:, a * 128:(a + 1) * 128], wbuf[m, a, :, first:first + size], preferred_element_type=F32
            )
        return total.astype(BF16).reshape(NZ, 32, size)

    halves = ((pq0, zq0), (pq1, zq1))

    def q_copy(i, d):
        to = (z + d) % NZ
        return remote(halves[i][0].at[to], halves[i][1].at[d], qs.at[i, d], qr.at[i, d], kv_0=to)

    def kv_copy(m, d):
        to = (z + d) % NZ
        return remote(pkv.at[m, to], zkv.at[m, d], ks.at[m, d], kr.at[m, d], kv_0=to)

    pq0[:, :, 0:256] = product(0)
    for d in FAR_FIRST:
        q_copy(0, d).start()
    pq1[...] = product(1)
    for d in FAR_FIRST:
        q_copy(1, d).start()
    pkv[0] = product(2)

    totals = []
    for i in range(2):
        total = halves[i][0][z].astype(F32)
        for d in Z_STEPS:
            q_copy(i, d).wait_recv()
            total += halves[i][1][d].astype(F32)
        totals.append(total)
    power = jnp.sum(totals[0][:, 256:384], axis=-1, keepdims=True)
    scale = lax.rsqrt(power / D + 1e-06)

    def turned(block):
        return block * cos + pltpu.roll(block, 64, 1) * sin

    for v in range(4):
        cols = slice(v * 128, (v + 1) * 128)
        block = turned(totals[v // 2][:, v % 2 * 128:v % 2 * 128 + 128] * scale).astype(BF16)
        qg[z, y, 0, :, cols] = block[0:16]
        qg[z, y, 1, :, cols] = block[16:32]
    q_start, q_hand_on, q_arrived, _, _, q_end = gather_2d(qg, z, y, azs, azr, ays, ayr, False)
    q_start(Z_STEPS[:2])
    for d in FAR_FIRST:
        kv_copy(0, d).start()
    q_start(Z_STEPS[2:], False)
    def finished(m):
        total = pkv[m, z].astype(F32)
        for d in Z_STEPS:
            kv_copy(m, d).wait_recv()
            total += zkv[m, d].astype(F32)
        for v in range(4):
            block = total[:, v * 128:(v + 1) * 128] * scale
            if m == 0:
                block = turned(block)
            at = m * 512 + v * 128
            kvown[:, at:at + 128] = block.astype(BF16)
            turn[m, pl.ds((v % 2) * 2 + v // 2 if m else v, 32, stride=4), :] = block

    upper = z >= NZ // 2

    pairs = ((knew, kg), (vnew, vg))

    def up_z(m, d):
        return remote(pairs[m][0], pairs[m][1].at[z, y], kzs.at[m, d], kzr.at[m, d], kv_0=(z + d) % NZ)

    def up_y(m, k, e):
        block = pairs[m][1].at[(z + NZ - k) % NZ, y]
        return remote(block, block, kys.at[m, k, e - 1], kyr.at[m, k, e - 1], kv_1=(y + e) % NY)

    own_up = [pltpu.make_async_copy(pairs[m][0], pairs[m][1].at[z, y], ls.at[6 + m]) for m in range(2)]

    def relay(m, k):
        at, to = (z + NZ - k) % NZ, (y + (1, 3)[k % 2]) % NY
        block = pairs[m][1].at[at, (y + (3, 1)[k % 2]) % NY]
        return remote(block, block, kys.at[m, k, 1], kyr.at[m, k, 1], kv_1=to)

    def to_upper(m, act):
        for d in Z_STEPS:
            @pl.when((z + d) % NZ >= NZ // 2)
            def _():
                act(up_z(m, d))

    def go_up(m):
        to_upper(m, lambda copy: copy.start())

        @pl.when(upper)
        def _():
            own_up[m].start()

    def hand_up(m):
        @pl.when(upper)
        def _():
            own_up[m].wait()
            for k in (0, *Z_STEPS):
                if k:
                    up_z(m, k).wait_recv()
                for e in (1, 3):
                    up_y(m, k, e).start()

    def hand_over(m):
        @pl.when(upper)
        def _():
            for k in (0, *Z_STEPS):
                up_y(m, k, (1, 3)[k % 2]).wait_recv()
                relay(m, k).start()

    def queries_of(zc, s):
        return jnp.concatenate(
            [qg[zc, i, s, :, (h * 2 + m) * 128:(h * 2 + m + 1) * 128] for m in range(2) for i in range(NY) for h in range(2)],
            axis=0,
        )

    odd = lax.broadcasted_iota(jnp.int32, (8, 128), 0) % 2 == 1
    offset = (z * NY + y) * 32

    def nth(step):
        return jnp.where(step % 2 == 1, (step + 1) // 2, (NZ - step // 2) % NZ)

    def attend(step, carry):
        k = nth(step)
        q_arrived(k)
        zc = (z + NZ - k) % NZ
        for s in range(2):
            b = 2 * zc + s
            limit = length[b] + accepted[b] - offset
            both = contract(kc[b], queries_of(zc, s), ((1,), (1,)))
            both = both.reshape(64, 8, 256)
            live = (code[...] < limit).reshape(64, 8, 128)
            score = jnp.where(odd[None], both[:, :, 128:], both[:, :, :128]) * ROOT
            score = jnp.where(live, score, NEG_FILL)
            top = jnp.max(score, axis=0)
            peaks = [jnp.max(jnp.where(odd == bool(m), top, NEG_FILL), axis=0, keepdims=True) for m in range(2)]
            peak = jnp.where(odd, peaks[1], peaks[0])
            grown = jnp.where(live, jnp.exp(score - peak[None]), 0.0)
            part = jnp.sum(grown, axis=0)
            for m in range(2):
                st[0, zc, 2 * s + m:2 * s + m + 1] = peaks[m]
                st[1, zc, 2 * s + m:2 * s + m + 1] = jnp.sum(jnp.where(odd == bool(m), part, 0.0), axis=0, keepdims=True)
            pscr[s] = grown.reshape(512, 128)
            chance = jnp.concatenate([pscr[s, pl.ds(m, 256, stride=2), :] for m in range(2)], axis=1).astype(BF16)
            acc[zc, s] = contract(chance, vc[b], ((0,), (0,))).astype(BF16)
        return carry

    for d in Z_STEPS[:2]:
        q_hand_on(d)
    loads[0].wait()
    loads[1].wait()
    lax.fori_loop(0, 3, attend, 0)
    for d in Z_STEPS[2:]:
        q_hand_on(d)
    finished(0)
    knew[...] = turn[0].astype(BF16).reshape(32, 4, 128)
    go_up(0)
    pkv[1] = product(3)
    for d in Z_STEPS:
        kv_copy(1, d).start()

    lax.fori_loop(3, NZ, attend, 0)
    q_end()

    weights = []
    head_row = 2 * y + lax.broadcasted_iota(jnp.int32, (32, 128), 0) // 16
    head_lane = lax.broadcasted_iota(jnp.int32, (32, 128), 1) // 16
    for s in range(2):
        rows = slice(s * 16, (s + 1) * 16)
        keys = jnp.concatenate(
            [kvown[rows, (h * 2 + m) * 128:(h * 2 + m + 1) * 128] for m in range(2) for h in range(2)], axis=0
        )
        both = contract(keys, queries_of(z, s), ((1,), (1,)))
        live = (head_row == head_lane) & (jnp.concatenate([seen[s], seen[s]], axis=0) > 0.5)
        chance = []
        for m in range(2):
            score = jnp.where(live, both[m * 32:(m + 1) * 32, m * 128:(m + 1) * 128] * ROOT, NEG_FILL)
            peak = jnp.max(score, axis=0, keepdims=True)
            grown = jnp.where(live, jnp.exp(score - peak), 0.0)
            sx[0, 2 * s + m:2 * s + m + 1] = peak
            sx[1, 2 * s + m:2 * s + m + 1] = jnp.sum(grown, axis=0, keepdims=True)
            chance.append(grown)
        weights.append(jnp.concatenate(chance, axis=1).astype(BF16))
    def log_sum(peak, total):
        return peak + jnp.log(jnp.maximum(total, 1e-30))

    def joined(parts):
        peak = functools.reduce(jnp.maximum, parts)
        return log_sum(peak, sum(jnp.exp(part - peak) for part in parts))

    mst[...] = log_sum(st[0], st[1])
    mst[z] = joined([mst[z], log_sum(sx[0], sx[1])])

    def st_copy(e):
        return remote(mst, yst.at[e], ss.at[e], sr.at[e], kv_1=(y + e) % NY)

    for e in Y_STEPS:
        st_copy(e).start()
    hand_up(0)
    parts = [mst[...]]
    for e in Y_STEPS:
        st_copy(e).wait_recv()
        parts.append(yst[e])
    zst[0] = joined(parts)

    def st_z(d):
        return remote(zst.at[0], zst.at[d], s2.at[d], r2.at[d], kv_0=(z + d) % NZ)

    for d in FAR_FIRST:
        st_z(d).start()
    finished(1)
    vnew[...] = turn[1].astype(BF16).reshape(32, 2, 2, 128)
    go_up(1)
    for s in range(2):
        rows = slice(s * 16, (s + 1) * 16)
        values = jnp.concatenate([kvown[rows, 512:768], kvown[rows, 768:1024]], axis=0)
        accx[s] = contract(weights[s], values, ((0,), (0,))).astype(BF16)
    hand_over(0)
    row = lax.broadcasted_iota(jnp.int32, (128, 128), 0)
    lane = lax.broadcasted_iota(jnp.int32, (128, 128), 1)
    same = row == lane
    lane = lax.broadcasted_iota(jnp.int32, (1, 128), 1) // 16
    lam = jnp.zeros((1, 128), F32)
    for h in range(8):
        lam = jnp.where(lane == h, -lambdas[h], lam)
    for d in Z_STEPS:
        st_z(d).wait_recv()
    gst[...] = joined([zst[d] for d in range(NZ)])

    def b_copy(zc, e):
        to = (y + e) % NY
        return remote(bs.at[to, zc], ybuf.at[e - 1, zc], bss.at[zc, e - 1], bsr.at[zc, e - 1], kv_1=to)

    def send_z(d):
        to = (z + d) % NZ
        return remote(zsum.at[to], zbuf.at[d], zs.at[d], zr.at[d], kv_0=to)

    def mixing(peaks, zc, s):
        ratio = jnp.exp(peaks - gst[zc])
        first = jnp.where(same, ratio[2 * s:2 * s + 1], 0.0)
        second = jnp.where(same, ratio[2 * s + 1:2 * s + 2] * lam, 0.0)
        return jnp.concatenate([first, second], axis=1).astype(BF16)

    def send_blocks(zc, last):
        for s in range(2):
            block = jnp.dot(mixing(st[0, zc], zc, s), acc[zc, s], preferred_element_type=F32)
            if last:
                block += jnp.dot(mixing(sx[0], zc, s), accx[s], preferred_element_type=F32)
            block = block.astype(BF16)
            for i in range(NY):
                bs[i, zc, s] = block[i * 32:(i + 1) * 32]
        for e in Y_STEPS:
            b_copy(zc, e).start()

    def blocks(d, carry):
        send_blocks((z + d) % NZ, False)
        return carry

    lax.fori_loop(1, NZ, blocks, 0)
    send_blocks(z, True)
    def sums(d, carry):
        zc = (z + d) % NZ
        total = bs[y, zc].astype(F32)
        for e in Y_STEPS:
            b_copy(zc, e).wait_recv()
            total += ybuf[e - 1, zc].astype(F32)
        zsum[zc] = total.astype(BF16)

        @pl.when(d < NZ)
        def _():
            send_z(d).start()

        return carry

    lax.fori_loop(1, NZ + 1, sums, 0)
    hand_up(1)
    total = zsum[z].astype(F32)
    for d in range(1, NZ):
        send_z(d).wait_recv()
        total += zbuf[d].astype(F32)
    norm = total * lax.rsqrt(jnp.mean(total * total, axis=-1, keepdims=True) + 1e-05)
    mg[z, y] = (norm * sub[...].astype(F32).reshape(1, 256) * LAMBDA_SCALE).astype(BF16)
    m_start, m_hand_on, m_arrived, _, _, m_end = gather_2d(mg, z, y, azs, azr, ays, ayr, False)
    r_start, r_hand_on, _, r_hand_over, r_handed_over, r_end = gather_2d(mg, z, y, azs, azr, ays, ayr, True)
    @pl.when(upper)
    def _():
        r_start()
        for d in Z_STEPS:
            r_hand_on(d)
        for k in (0, *Z_STEPS):
            r_hand_over(k)

    @pl.when(z < NZ // 2)
    def _():
        m_start()
        for d in Z_STEPS:
            m_hand_on(d)

    hand_over(1)
    loads[2].wait()

    @pl.when(upper)
    def _():
        for k in (0, *Z_STEPS):
            r_handed_over(k)

    @pl.when(z < NZ // 2)
    def _():
        for k in (0, *Z_STEPS):
            m_arrived(k)

    result = jnp.zeros((256, 128), F32)
    for h in range(8):
        i, k = h // 2, h % 2
        rows = jnp.concatenate(
            [mg[a, i, s, k * 16:(k + 1) * 16] for a in range(NZ) for s in range(2)], axis=0
        )
        result += jnp.dot(rows, wo[h * 256:(h + 1) * 256], preferred_element_type=F32)
    prod[...] = result.astype(BF16)
    swap = remote(prod, got, xs, xr, tp=1 - c)
    swap.start()
    swap.wait()
    result = prod[...].astype(F32) + got[...].astype(F32)
    out[...] = jnp.where(c == 0, result[:, 0:64], result[:, 64:128]).astype(BF16)

    for e in Y_STEPS:
        gain_copy(e).wait_send()
        tok_copy(e).wait_send()
        st_copy(e).wait_send()
        for i in range(4):
            w_copy(i, e).wait_send()
    for d in Z_STEPS:
        for i in range(2):
            q_copy(i, d).wait_send()
        for m in range(2):
            kv_copy(m, d).wait_send()
        st_z(d).wait_send()
        send_z(d).wait_send()

    pl.when(upper)(r_end)
    pl.when(z < NZ // 2)(m_end)
    for m in range(2):
        to_upper(m, lambda copy: copy.wait_send())

    def drain(zc, carry):
        for e in Y_STEPS:
            b_copy(zc, e).wait_send()
        return carry

    lax.fori_loop(0, NZ, drain, 0)

    @pl.when(upper)
    def _():
        for m in range(2):
            for k in (0, *Z_STEPS):
                up_y(m, k, 1).wait_send()
                up_y(m, k, 3).wait_send()
                up_y(m, k, (3, 1)[k % 2]).wait_recv()
                relay(m, k).wait()


def layer(*operands):
    vmem, smem = pl.BlockSpec(memory_space=pltpu.VMEM), pl.BlockSpec(memory_space=pltpu.SMEM)
    anywhere = pl.BlockSpec(memory_space=pltpu.HBM)
    y_pair, z_pair = [DMA((NY,))] * 2, [DMA((NZ,))] * 2
    zy_pair = [DMA((NZ, NY - 1))] * 2
    return pl.pallas_call(
        layer_kernel,
        name="layer",
        out_shape=(
            jax.ShapeDtypeStruct((256, 64), BF16),
            jax.ShapeDtypeStruct((NZ, NY, 32, 4, 128), BF16),
            jax.ShapeDtypeStruct((NZ, NY, 32, 2, 2, 128), BF16),
        ),
        in_specs=[smem] * 3 + [vmem] * 8 + [anywhere] * 3,
        out_specs=(vmem, anywhere, anywhere),
        scratch_shapes=[
            pltpu.VMEM((NY, 256, 128), BF16),
            pltpu.VMEM((NY, 16, 128), BF16),
            pltpu.VMEM((3, NY, 128, 512), BF16),
            pltpu.VMEM((256, 512), BF16),
            pltpu.VMEM((NZ, 32, 384), BF16),
            pltpu.VMEM((NZ, 32, 256), BF16),
            pltpu.VMEM((2, NZ, 32, 512), BF16),
            pltpu.VMEM((NZ, 32, 384), BF16),
            pltpu.VMEM((NZ, 32, 256), BF16),
            pltpu.VMEM((2, NZ, 32, 512), BF16),
            pltpu.VMEM((NZ, NY, 2, 16, 512), BF16),
            pltpu.VMEM((32, 1024), BF16),
            pltpu.VMEM((32, 4, 128), BF16),
            pltpu.VMEM((32, 2, 2, 128), BF16),
            pltpu.VMEM((2, 128, 128), F32),
            pltpu.VMEM((16, 512, 128), BF16),
            pltpu.VMEM((16, 256, 256), BF16),
            pltpu.VMEM((2048, 128), BF16),
            pltpu.VMEM((512, 128), jnp.int32),
            pltpu.VMEM((2, 512, 128), F32),
            pltpu.VMEM((2, NZ, 4, 128), F32),
            pltpu.VMEM((2, 4, 128), F32),
            pltpu.VMEM((NZ, 4, 128), F32),
            pltpu.VMEM((NZ, 2, 256, 256), BF16),
            pltpu.VMEM((2, 256, 256), BF16),
            pltpu.VMEM((NY, NZ, 4, 128), F32),
            pltpu.VMEM((NZ, NZ, 4, 128), F32),
            pltpu.VMEM((NZ, 4, 128), F32),
            pltpu.VMEM((NY, NZ, 2, 32, 256), BF16),
            pltpu.VMEM((NY - 1, NZ, 2, 32, 256), BF16),
            pltpu.VMEM((NZ, 2, 32, 256), BF16),
            pltpu.VMEM((NZ, 2, 32, 256), BF16),
            pltpu.VMEM((NZ, NY, 2, 32, 256), BF16),
            pltpu.VMEM((256, 128), BF16),
            pltpu.VMEM((256, 128), BF16),
            DMA((8,)), DMA((4, NY)), DMA((4, NY)), *y_pair, *y_pair,
            DMA((2, NZ)), DMA((2, NZ)), DMA((2, NZ)), DMA((2, NZ)),
            *z_pair, DMA((NZ, NY)), DMA((NZ, NY)), DMA((2, NZ)), DMA((2, NZ)), DMA((2, NZ, NY - 1)), DMA((2, NZ, NY - 1)),
            *y_pair, *z_pair, *zy_pair, *z_pair, DMA, DMA,
        ],
        compiler_params=pltpu.CompilerParams(
            collective_id=0, has_side_effects=True, vmem_limit_bytes=56 * 1024 * 1024
        ),
    )(*operands)


def insert_kernel(length, accepted, k_in, v_in, kg, vg, ko, vo, kt, vt, ins, new, outs):
    z, y, _ = places()
    offset = (z * NY + y) * 32

    def group(g):
        return pl.ds(g * 4, 4)

    def load(g):
        return (
            pltpu.make_async_copy(k_in.at[group(g)], kt.at[group(g), 16:48], ins.at[0, g]),
            pltpu.make_async_copy(v_in.at[group(g)], vt.at[group(g), 16:48], ins.at[1, g]),
        )

    def place(b):
        at = pl.ds(jnp.clip(length[b] + accepted[b] - offset + 16, 0, 48), 16)
        rows = pl.ds((b % 2) * 16, 16)
        return [
            pltpu.make_async_copy(kg.at[b // 2, i, rows], kt.at[b, at, i], new.at[0, b, i]) for i in range(NY)
        ] + [
            pltpu.make_async_copy(vg.at[b // 2, i, rows], vt.at[b, at, :, i], new.at[1, b, i]) for i in range(NY)
        ]

    def store(g):
        return (
            pltpu.make_async_copy(kt.at[group(g), 16:48], ko.at[group(g)], outs.at[0, g]),
            pltpu.make_async_copy(vt.at[group(g), 16:48], vo.at[group(g)], outs.at[1, g]),
        )

    def act(copies, name):
        for copy in copies:
            getattr(copy, name)()

    for g in range(4):
        act(load(g), "start")

    @pl.when(z >= NZ // 2)
    def _():
        for g in range(4):
            act(load(g), "wait")
            for b in range(4 * g, 4 * g + 4):
                act(place(b), "start")
        for g in range(4):
            for b in range(4 * g, 4 * g + 4):
                act(place(b), "wait")
            act(store(g), "start")

    @pl.when(z < NZ // 2)
    def _():
        for g in range(4):
            act(load(g), "wait")
            act(store(g), "start")

    for g in range(4):
        act(store(g), "wait")


def insert(length, accepted, keys, values, new_keys, new_values):
    smem, anywhere = pl.BlockSpec(memory_space=pltpu.SMEM), pl.BlockSpec(memory_space=pltpu.HBM)
    return pl.pallas_call(
        insert_kernel,
        name="insert",
        in_specs=[smem] * 2 + [anywhere] * 4,
        out_specs=(anywhere, anywhere),
        scratch_shapes=[
            pltpu.VMEM((16, 64, NY, 4, 128), BF16), pltpu.VMEM((16, 64, 2, NY, 2, 128), BF16),
            DMA((2, 4)), DMA((2, 16, NY)), DMA((2, 4)),
        ],
        out_shape=(
            jax.ShapeDtypeStruct((16, 32, NY, 4, 128), BF16),
            jax.ShapeDtypeStruct((16, 32, 2, NY, 2, 128), BF16),
        ),
        compiler_params=pltpu.CompilerParams(vmem_limit_bytes=62 * 1024 * 1024),
    )(length, accepted, keys, values, new_keys, new_values)


def per_device(tokens, in_gain, query_weight, key_weight, value_weight, out_weight, lambdas, sub_gain,
               key_cache, value_cache, cache_len, accepted, parents):
    frequency = np.float32(10000.0) ** (-np.arange(64, dtype=np.float32) / np.float32(64))
    frequency = jnp.asarray(np.concatenate([frequency, frequency])[None, :])
    output, new_keys, new_values = layer(
        cache_len, accepted, lambdas, parents, tokens.reshape(256, 128), in_gain.reshape(1, 128),
        sub_gain, frequency, query_weight, key_weight, value_weight,
        key_cache.reshape(16, 512, 128), value_cache.reshape(16, 256, 256), out_weight,
    )
    values = value_cache.reshape(16, 32, NY, 2, 2, 128).transpose(0, 1, 4, 2, 3, 5)
    key_out, value_out = insert(
        cache_len, accepted, key_cache.reshape(16, 32, NY, 4, 128), values, new_keys, new_values
    )
    value_out = value_out.transpose(0, 1, 3, 4, 2, 5).reshape(value_cache.shape)
    return output.reshape(16, 16, 64), key_out.reshape(key_cache.shape), value_out


def solution(mesh):
    torus = Mesh(mesh.devices.reshape(mesh.shape["dp"], NZ, NY, mesh.shape["tp"]), ("dp", "kv_0", "kv_1", "tp"))
    placed = (
        P("dp", None, KV), P(KV), P(KV, "tp"), P(KV, "tp"), P(KV, "tp"), P("tp", KV), P("tp"), P(),
        P("dp", KV, "tp", None, None), P("dp", KV, "tp", None), P("dp"), P("dp"), P("dp", None),
    )
    return jax.shard_map(
        per_device, mesh=torus, in_specs=placed,
        out_specs=(P("dp", None, KV_TP), P("dp", KV, "tp", None, None), P("dp", KV, "tp", None)),
        check_vma=False,
    )
```
